256 devices in a mesh: sp: 32 (over z, x), tp: 8 (over y, core).
Axes of the slice: x: 4, y: 4, z: 8, core: 2. Of those that a mesh axis runs over, the one named last changes fastest.
Arguments:
- tokens: bfloat16 [8192, 1024], P(('sp', 'tp')), may hold values from -6 to 6
- doc_ids: int32 [8192], P('sp'), may hold values from 0 to 31, never falling along the last dimension, each value on 1 to 4608 neighbouring positions
- down_query: bfloat16 [1024, 256], P('sp'), may hold values from -0.1875 to 0.1875
- down_key: bfloat16 [1024, 256], P('sp'), may hold values from -0.1875 to 0.1875
- down_rotary: bfloat16 [1024, 32], P('sp'), may hold values from -0.1875 to 0.1875
- query_gain: float32 [256], replicated, may hold values from 0.1 to 1.9
- key_gain: float32 [256], replicated, may hold values from 0.1 to 1.9
- up_query: bfloat16 [256, 1536], P('sp', 'tp'), may hold values from -0.375 to 0.375
- up_key: bfloat16 [256, 1024], P('sp', 'tp'), may hold values from -0.375 to 0.375
- up_value: bfloat16 [256, 1024], P('sp', 'tp'), may hold values from -0.375 to 0.375
- output_weight: bfloat16 [1024, 1024], P('tp', 'sp'), may hold values from -0.1875 to 0.1875
- out_gain: float32 [1024], replicated, may hold values from 0.1 to 1.9
Outputs:
- mixed: bfloat16 [8192, 1024], P(('sp', 'tp'))
- log_sums: float32 [8192, 16], P('sp', 'tp')
The draws below stay inside these ranges and needn't reach their ends.
Inputs may be any that keep to these rules, and one draw needn't show every extreme that they name: doc_ids never fall along the sequence and run from 0 to at most the number of devices along sp minus one; each document has 1 to 4608 positions, and one document has exactly that many.
All inputs are finite; a program needn't handle non-finite values.
Results may differ from the reference program's by a relative error of at most 0.02.
Values may be sent and summed in bfloat16 or wider, within the bound.
A program may use at most 64 MiB of HBM per device.

```python
import math
import jax
import jax.numpy as jnp
import numpy as np
from jax import lax

D = 1024
HEADS = 16
Q_RANK = 256
KV_RANK = 256
NOPE = 64
ROPE = 32
VDIM = 64
TOK_DEV = 256
TOKENS = 8192
N_SP = 32


def block_scale(key, extent, pieces, least, high):
    def one(position, shards_of):
        draws = jax.random.uniform(jax.random.fold_in(jax.random.fold_in(key, 6), position), (shards_of,), jnp.float32, least / len(pieces), high / len(pieces))
        return jnp.repeat(jnp.exp(draws), extent[position] // shards_of).reshape((-1,) + (1,) * (len(extent) - position - 1))

    level = one(*pieces[0])
    for cut in pieces[1:]:
        level = level * one(*cut)
    return level


def profile(number_of, total, bound, skew):
    portions = [(1 << 20) // math.isqrt(standing ** skew) + 1 for standing in range(2, number_of + 1)]
    rest, given = total - bound - (number_of - 1), [1] * (number_of - 1)
    while rest > 0:
        movable = [i for i in range(number_of - 1) if given[i] < bound]
        pool, budget = sum([portions[i] for i in movable]), rest
        for i in movable:
            more = min(bound - given[i], max(1, budget * portions[i] // pool), rest)
            given[i] = given[i] + more
            rest = rest - more
    return np.array([bound] + given)


def uneven_parts(key, count, total, bound, lean):
    if count == 2:
        one = jax.random.randint(key, (), max(1, total - bound), min(bound, total - 1) + 1)
        return jnp.stack([one, total - one])
    lengths = jnp.asarray(profile(count, total, bound, lean), jnp.int32)
    twos = (count - 1) // 2
    source_of, sink = lengths[1:1 + 2 * twos:2], lengths[2:2 + 2 * twos:2]
    room = jnp.minimum(source_of - 1, bound - sink)
    moved = jax.random.randint(jax.random.fold_in(key, 1), (twos,), 0, 1 << 20) % (room + 1)
    lengths = lengths.at[1:1 + 2 * twos:2].set(source_of - moved).at[2:2 + 2 * twos:2].set(sink + moved)
    return lengths[jax.random.permutation(jax.random.fold_in(key, 2), count)]


def normal_values(own_key, shape, width, bound, split=(), kind=jnp.bfloat16):
    values = width * jax.random.normal(own_key, shape, jnp.float32)
    if split:
        values = values * block_scale(own_key, shape, split, -0.22, 0.18)
    return jnp.clip(values, -bound, bound).astype(kind)


def setup_inputs(seed: int = 0) -> dict:
    seeds = jax.random.split(jax.random.key(seed), 13)
    return {
        "tokens": normal_values(seeds[0], (TOKENS, D), 1.0, 6.0, ((0, 256),)),
        "doc_ids": jnp.searchsorted(jnp.cumsum(uneven_parts(seeds[1], N_SP, TOKENS, TOK_DEV * N_SP // 2 + 2 * TOK_DEV, 2)), jnp.arange(TOKENS), side="right").astype(jnp.int32),
        "down_query": normal_values(seeds[2], (D, Q_RANK), D ** -0.5, 0.1875, ((0, 32),)),
        "down_key": normal_values(seeds[3], (D, KV_RANK), D ** -0.5, 0.1875, ((0, 32),)),
        "down_rotary": normal_values(seeds[4], (D, ROPE), D ** -0.5, 0.1875, ((0, 32),)),
        "query_gain": jnp.clip(1.0 + 0.18 * jax.random.normal(seeds[5], (Q_RANK,), jnp.float32), 0.1, 1.9),
        "key_gain": jnp.clip(1.0 + 0.18 * jax.random.normal(seeds[6], (KV_RANK,), jnp.float32), 0.1, 1.9),
        "up_query": normal_values(seeds[7], (Q_RANK, HEADS * (NOPE + ROPE)), Q_RANK ** -0.5, 0.375, ((0, 32), (1, 8))),
        "up_key": normal_values(seeds[8], (KV_RANK, HEADS * NOPE), KV_RANK ** -0.5, 0.375, ((0, 32), (1, 8))),
        "up_value": normal_values(seeds[9], (KV_RANK, HEADS * VDIM), KV_RANK ** -0.5, 0.375, ((0, 32), (1, 8))),
        "output_weight": normal_values(seeds[10], (HEADS * VDIM, D), (HEADS * VDIM) ** -0.5, 0.1875, ((0, 8), (1, 32))),
        "out_gain": jnp.clip(1.0 + 0.18 * jax.random.normal(seeds[11], (D,), jnp.float32), 0.1, 1.9),
    }


NEG_BIG = -1e+30
THETA = 10000.0
EPS = 1e-06

def settle(quantity):
    return lax.optimization_barrier(quantity.astype(jnp.bfloat16))

def rms_gain(summed, gain_vector):
    widened = settle(summed).astype(jnp.float32)
    scaled = widened * lax.rsqrt(lax.optimization_barrier(jnp.mean(widened * widened, axis=-1, keepdims=True)) + EPS)
    return (scaled * gain_vector).astype(jnp.bfloat16)

def rotate(vectors, positions):
    half_width = vectors.shape[-1] // 2
    inverse = THETA ** (-jnp.arange(half_width, dtype=jnp.float32) / half_width)
    angles = positions.astype(jnp.float32)[:, None] * inverse[None, :]
    angles = angles.reshape((vectors.shape[0],) + (1,) * (vectors.ndim - 2) + (half_width,))
    cosine_part = jnp.cos(angles)
    sine_part = jnp.sin(angles)
    widened = vectors.astype(jnp.float32)
    front_half = widened[..., :half_width]
    back_half = widened[..., half_width:]
    return jnp.concatenate([front_half * cosine_part - back_half * sine_part, back_half * cosine_part + front_half * sine_part], axis=-1).astype(jnp.bfloat16)

def reference(tokens, doc_ids, down_query, down_key, down_rotary, query_gain, key_gain, up_query, up_key, up_value, output_weight, out_gain):
    highest = lax.Precision.HIGHEST
    positions = jnp.arange(TOKENS, dtype=jnp.int32)
    query_latent = rms_gain(jnp.dot(tokens, down_query, preferred_element_type=jnp.float32), query_gain)
    key_latent = rms_gain(jnp.dot(tokens, down_key, preferred_element_type=jnp.float32), key_gain)
    key_turned = rotate(settle(jnp.dot(tokens, down_rotary, preferred_element_type=jnp.float32)), positions)
    queries = settle(jnp.dot(query_latent, up_query, preferred_element_type=jnp.float32))
    queries = queries.reshape(TOKENS, HEADS, NOPE + ROPE)
    query_plain = queries[..., :NOPE]
    query_turned = rotate(queries[..., NOPE:], positions)
    key_plain = settle(jnp.dot(key_latent, up_key, preferred_element_type=jnp.float32)).reshape(TOKENS, HEADS, NOPE)
    values = settle(jnp.dot(key_latent, up_value, preferred_element_type=jnp.float32)).reshape(TOKENS, HEADS, VDIM)
    score_scale = 1.0 / math.sqrt(NOPE + ROPE)
    plain_wide = key_plain.astype(jnp.float32)
    turned_wide = key_turned.astype(jnp.float32)
    values_wide = values.astype(jnp.float32)

    def one_block(block_parts):
        plain_block, turned_block, docs_block = block_parts
        scores = jnp.einsum('qhd,khd->hqk', plain_block.astype(jnp.float32), plain_wide, precision=highest)
        scores = scores + jnp.einsum('qhr,kr->hqk', turned_block.astype(jnp.float32), turned_wide, precision=highest)
        scores = scores * score_scale
        same_doc = (docs_block[:, None] == doc_ids[None, :])[None]
        top_score = lax.optimization_barrier(jnp.max(jnp.where(same_doc, scores, NEG_BIG), axis=-1, keepdims=True))
        weights = jnp.where(same_doc, jnp.exp(scores - top_score), 0.0)
        weight_sum = lax.optimization_barrier(jnp.sum(weights, axis=-1))
        mixed_rows = jnp.einsum('hqk,khv->qhv', settle(weights).astype(jnp.float32), values_wide, precision=highest)
        mixed_rows = mixed_rows / weight_sum.T[:, :, None]
        return (mixed_rows, (top_score[..., 0] + jnp.log(weight_sum)).T)
    blocks = (query_plain.reshape(N_SP, TOK_DEV, HEADS, NOPE), query_turned.reshape(N_SP, TOK_DEV, HEADS, ROPE), doc_ids.reshape(N_SP, TOK_DEV))
    mixed_rows, log_sums = lax.map(one_block, blocks)
    attended = mixed_rows.reshape(TOKENS, HEADS * VDIM).astype(jnp.bfloat16)
    log_sums = log_sums.reshape(TOKENS, HEADS)
    projected = jnp.dot(attended, output_weight, preferred_element_type=jnp.float32)
    return (rms_gain(projected, out_gain), log_sums)
```

```python
import functools
import math

import jax
import jax.numpy as jnp
from jax import lax
from jax.experimental import pallas as pl
from jax.experimental.pallas import tpu as pltpu
from jax.sharding import PartitionSpec as P

NOPE = 64
ROPE = 32
THETA = 10000.0
EPS = 1e-06
UNSEEN = -1e30
MASKED = -3e38
SCALE = 1.0 / math.sqrt(NOPE + ROPE)
SCALE_2 = SCALE * math.log2(math.e)
MESH = pl.DeviceIdType.MESH
F32 = jnp.float32
BF16 = jnp.bfloat16

STEPS = (0, 1, -1, 2, -2, 3, -3, 4)
SLOT_OF = {0: 0, 1: 1, -1: 2, 2: 3, -2: 4, 3: 5, -3: 6, 4: 7, -4: 7}
GROUPS = ((0, 4), (4, 4))


def slot8(r):
    late = r // 5
    return (1 - late) * (2 * r - 1 + (8 - r) // 8) + late * (16 - 2 * r)


def slot4(r):
    return 2 * r - r // 2 - 4 * (r // 3)


def nt(a, b):
    return lax.dot_general(a, b, (((1,), (1,)), ((), ())), preferred_element_type=F32)


def nn(a, b):
    return jnp.dot(a, b, preferred_element_type=F32)


def body(
    tok,
    wpiece,
    bundle,
    qdoc,
    kdoc,
    cos_q,
    sin_q,
    cos_k,
    sin_k,
    query_gain,
    key_gain,
    out_gain,
    mixed,
    log_sums,
    wbuf,
    bbuf,
    kbuf,
    qlbuf,
    w_down,
    w_rot,
    w_uq,
    w_uk,
    w_uv,
    w_out,
    kx_w,
    vt_w,
    qx,
    top,
    total,
    acc,
    partial,
    rsbuf,
    send_z,
    recv_z,
    send_2,
    recv_2,
    send_3,
    recv_3,
    send_p,
    recv_p,
    send_bz,
    recv_bz,
    send_bx,
    recv_bx,
    send_t,
    recv_t,
):
    sp = lax.axis_index("sp")
    tp = lax.axis_index("tp")
    z, x = sp // 4, sp % 4
    y, c = tp // 2, tp % 2

    def chip(dz=0, dx=0, dy=0, flip=False):
        core = 1 - c if flip else c
        return (((z + dz + 8) % 8) * 4 + (x + dx + 4) % 4, ((y + dy + 4) % 4) * 2 + core)

    def along_2(d):
        return chip(dx=(1 - c) * d, dy=c * d)

    def along_3(d):
        return chip(dx=c * d, dy=(1 - c) * d)

    tp_peers = [(dy, flip) for dy in (1, 3, 2, 0) for flip in (False, True) if (dy, flip) != (0, False)]

    barrier = pltpu.get_barrier_semaphore()
    peers = [chip(dz=d) for d in STEPS[1:]] + [chip(dx=1), chip(dx=-1)]
    peers += [chip(dy=dy, flip=flip) for dy, flip in tp_peers]
    for peer in peers:
        pl.semaphore_signal(barrier, inc=1, device_id=peer, device_id_type=MESH)
    pl.semaphore_wait(barrier, len(peers))

    started = []

    def push(src, dst, ssem, rsem, peer):
        copy = pltpu.make_async_remote_copy(
            src_ref=src, dst_ref=dst, send_sem=ssem, recv_sem=rsem, device_id=peer, device_id_type=MESH
        )
        copy.start()
        started.append(copy)

    def landed(dst, rsem):
        pltpu.make_async_remote_copy(
            src_ref=dst, dst_ref=dst, send_sem=rsem, recv_sem=rsem, device_id=chip(flip=True), device_id_type=MESH
        ).wait_recv()

    def spread(ids, buf, first):
        n2, n3 = 6 * ids, 24 * ids

        def go_z():
            for k in range(1, 8):
                slot = SLOT_OF[-STEPS[k]]
                push(first, buf.at[0, 0, 0, slot], send_z.at[ids, k - 1], recv_z.at[ids, slot - 1], chip(dz=STEPS[k]))

        def wait_z(g):
            lo, n = GROUPS[g]
            for k in range(max(lo, 1), lo + n):
                landed(buf.at[0, 0, 0, k], recv_z.at[ids, k - 1])

        def send_2nd(a_from, a_to, g, d):
            lo, n = GROUPS[g]
            i = n2 + (a_to - 1) * 2 + g
            push(buf.at[0, 0, a_from, pl.ds(lo, n)], buf.at[0, 0, a_to, pl.ds(lo, n)], send_2.at[i], recv_2.at[i], along_2(d))

        def wait_2nd(a, g):
            lo, n = GROUPS[g]
            landed(buf.at[0, 0, a, pl.ds(lo, n)], recv_2.at[n2 + (a - 1) * 2 + g])

        def send_3rd(b_from, b_to, a, g, d):
            lo, n = GROUPS[g]
            i = n3 + ((b_to - 1) * 4 + a) * 2 + g
            push(buf.at[0, b_from, a, pl.ds(lo, n)], buf.at[0, b_to, a, pl.ds(lo, n)], send_3.at[i], recv_3.at[i], along_3(d))

        def wait_3rd(b, a, g):
            lo, n = GROUPS[g]
            landed(buf.at[0, b, a, pl.ds(lo, n)], recv_3.at[n3 + ((b - 1) * 4 + a) * 2 + g])

        def share(b, a, g):
            lo, n = GROUPS[g]
            i = 32 * ids + (b * 4 + a) * 2 + g
            push(buf.at[0, b, a, pl.ds(lo, n)], buf.at[1, b, a, pl.ds(lo, n)], send_p.at[i], recv_p.at[i], chip(flip=True))

        def shared(b, a, g):
            lo, n = GROUPS[g]
            landed(buf.at[1, b, a, pl.ds(lo, n)], recv_p.at[32 * ids + (b * 4 + a) * 2 + g])

        def onward(a, g):
            send_3rd(0, 1, a, g, 1)
            send_3rd(0, 2, a, g, -1)
            share(0, a, g)

        def plane():
            for g in range(2):
                wait_z(g)
                send_2nd(0, 1, g, 1)
                send_2nd(0, 2, g, -1)
                onward(0, g)
            for g in range(2):
                wait_2nd(1, g)
                if g == 0:
                    send_2nd(1, 3, g, 1)
                onward(1, g)
                wait_2nd(2, g)
                if g == 1:
                    send_2nd(2, 3, g, -1)
                onward(2, g)
            for g in range(2):
                wait_2nd(3, g)
                onward(3, g)

        def near(a):
            for g in range(2):
                wait_3rd(1, a, g)
                if g == 0:
                    send_3rd(1, 3, a, g, 1)
                share(1, a, g)
                wait_3rd(2, a, g)
                if g == 1:
                    send_3rd(2, 3, a, g, -1)
                share(2, a, g)

        def far(a):
            for g in range(2):
                wait_3rd(3, a, g)
                share(3, a, g)

        def partner(b, a):
            for g in range(2):
                shared(b, a, g)

        return go_z, plane, near, far, partner

    go_z, plane, near, far, partner = spread(0, wbuf, wpiece)
    go_z()
    wbuf[0, 0, 0, 0] = wpiece[...]
    for k in range(1, 8):
        slot = SLOT_OF[-STEPS[k]]
        push(bundle, bbuf.at[0, slot], send_bz.at[k - 1], recv_bz.at[slot - 1], chip(dz=STEPS[k]))
    bbuf[0, 0] = bundle[...]
    plane()
    for k in range(1, 8):
        landed(bbuf.at[0, k], recv_bz.at[k - 1])
    for d, a in ((1, 1), (-1, 2)):
        push(bbuf.at[0], bbuf.at[a], send_bx.at[a - 1], recv_bx.at[a - 1], chip(dx=d))
    for a in range(4):
        near(a)
    for a in range(4):
        far(a)
    landed(bbuf.at[1], recv_bx.at[0])
    push(bbuf.at[1, pl.ds(0, 4)], bbuf.at[3, pl.ds(0, 4)], send_bx.at[2], recv_bx.at[2], chip(dx=1))
    landed(bbuf.at[2], recv_bx.at[1])
    push(bbuf.at[2, pl.ds(4, 4)], bbuf.at[3, pl.ds(4, 4)], send_bx.at[3], recv_bx.at[3], chip(dx=-1))
    for b in range(4):
        for a in range(4):
            partner(b, a)
    landed(bbuf.at[3, pl.ds(0, 4)], recv_bx.at[2])
    landed(bbuf.at[3, pl.ds(4, 4)], recv_bx.at[3])

    lane32 = lax.broadcasted_iota(jnp.int32, (1, 4, 1, 128), 3) // 32
    quarter = (lane32 == lax.broadcasted_iota(jnp.int32, (1, 4, 1, 128), 1)).astype(F32)[0]

    def arrange(s, carry):
        kz = slot8((s // 4 - z + 8) % 8)
        kx = slot4((s % 4 - x + 4) % 4)
        for half, first in ((0, c), (1, 1 - c)):
            for u in range(2):
                rows = []
                for yy in range(4):
                    ky = slot4((yy - y + 4) % 4)
                    b, a = (ky, kx) if half == 0 else (kx, ky)
                    rows.append(wbuf[first, b, a, kz, u].astype(F32))
                w_down[pl.ds(pl.multiple_of(s * 32, 32), 32), pl.ds((2 * half + u) * 128, 128)] = jnp.concatenate(
                    rows, axis=0
                ).astype(BF16)
        r = bbuf[kx, kz, 4].astype(F32)
        r = (r[None] * quarter).reshape(32, 128)
        w_rot[pl.ds(pl.multiple_of(s * 32, 32), 32), :] = r.astype(BF16)
        o = bbuf[kx, kz, pl.ds(5, 4)].astype(F32).reshape(32, 128)
        w_out[pl.ds(pl.multiple_of(s * 32, 32), 32), :] = o.astype(BF16)
        return carry

    lax.fori_loop(0, 32, arrange, 0)

    def arrange_up(s, carry):
        kz = slot8((s // 2 - z + 8) % 8)
        halves = [slot4((2 * (s % 2) + i - x + 4) % 4) for i in range(2)]
        at = pl.ds(pl.multiple_of(s * 16, 16), 16)
        for u in range(2):
            pair = [bbuf[kx, kz, u].astype(F32) for kx in halves]
            w_uq[at, pl.ds(u * 128, 128)] = jnp.concatenate(pair, axis=0).astype(BF16)
        w_uk[at, :] = jnp.concatenate([bbuf[kx, kz, 2].astype(F32) for kx in halves], axis=0)
        w_uv[at, :] = jnp.concatenate([bbuf[kx, kz, 3].astype(F32) for kx in halves], axis=0)
        return carry

    lax.fori_loop(0, 16, arrange_up, 0)

    own = tok[...]
    down = nn(own, w_down[...])

    def normed(v, gain):
        v = v.astype(BF16).astype(F32)
        return v * lax.rsqrt(jnp.mean(v * v, axis=-1, keepdims=True) + EPS) * gain

    latent_q = normed(down[:, :256], query_gain[...]).astype(BF16)
    latent_k = normed(down[:, 256:], key_gain[...]).astype(BF16)
    r = nn(own, w_rot[...])
    r = (r + pltpu.roll(r, 64, 1))
    r = (r + pltpu.roll(r, 32, 1)).astype(BF16).astype(F32)
    r = r * cos_k[...] + pltpu.roll(r, 16, 1) * sin_k[...]
    lane = lax.broadcasted_iota(jnp.int32, (16, 128), 1)
    in_a = lane < 32
    in_b = (lane >= 64) & (lane < 96)
    tail = jnp.where(in_a, r[:16], jnp.where(in_b, r[16:], kdoc[...])).astype(BF16)
    kbuf[0, 0, 0, 0, pl.ds(0, 32)] = latent_k[:, :128]
    kbuf[0, 0, 0, 0, pl.ds(32, 32)] = latent_k[:, 128:]
    kbuf[0, 0, 0, 0, pl.ds(64, 16)] = tail
    qlbuf[pl.ds(tp, 1)] = latent_q[None]

    go_z, plane, near, far, partner = spread(1, kbuf, kbuf.at[0, 0, 0, 0])
    go_z()
    for i, (dy, flip) in enumerate(tp_peers):
        push(qlbuf.at[tp], qlbuf.at[tp], send_t.at[i], recv_t.at[i], chip(dy=dy, flip=flip))

    lane = lax.broadcasted_iota(jnp.int32, (256, 128), 1)
    uk = w_uk[...]
    head0 = jnp.where(lane < 64, uk, 0.0).astype(BF16)
    head1 = jnp.where(lane < 64, pltpu.roll(uk, 64, 1), 0.0).astype(BF16)
    row = lax.broadcasted_iota(jnp.int32, (128, 128), 0)
    col = lax.broadcasted_iota(jnp.int32, (128, 128), 1)
    for g in range(2):
        pick = ((row - 64 * g == col - 64) & (col >= 64) & (col < 96)).astype(F32).astype(BF16)
        kx_w[g, pl.ds(0, 256), pl.ds(0, 128)] = head0
        kx_w[g, pl.ds(0, 256), pl.ds(128, 128)] = head1
        kx_w[g, pl.ds(256, 128), pl.ds(0, 128)] = pick
        kx_w[g, pl.ds(256, 128), pl.ds(128, 128)] = pick
    vt_w[...] = jnp.transpose(w_uv[...]).astype(BF16)
    top[...] = jnp.full_like(top, UNSEEN)
    total[...] = jnp.zeros_like(total)
    acc[...] = jnp.zeros_like(acc)

    plane()

    for i, (dy, flip) in enumerate(tp_peers):
        source = ((y + 4 - dy) % 4) * 2 + (1 - c if flip else c)
        landed(qlbuf.at[source], recv_t.at[i])
    q = nn(qlbuf[...].reshape(256, 256), w_uq[...]).astype(BF16).astype(F32)
    for h in range(2):
        v = q[:, 128 * h : 128 * h + 128]
        qx[h] = (v * cos_q[...] + pltpu.roll(v, 96, 1) * sin_q[...]).astype(BF16)

    row = lax.broadcasted_iota(jnp.int32, (128, 256), 0)
    doc_pick = [(row == 64 * g + 32).astype(F32).astype(BF16) for g in range(2)]

    def unit(side, b, a):
        block = kbuf[side, b, a]
        keys, docs, values = [], [], []
        for g in range(2):
            low = block[:, 16 * g : 16 * g + 16].reshape(128, 128)
            high = block[:, 32 + 16 * g : 48 + 16 * g].reshape(128, 128)
            rest = block[:, 64:80].reshape(128, 128)
            latent = jnp.concatenate([low, high], axis=1)
            keys.append(nn(jnp.concatenate([latent, rest], axis=1), kx_w[g]).astype(BF16))
            docs.append(nn(rest, doc_pick[g]))
            values.append(nt(vt_w[...], latent).astype(BF16))
        keys = jnp.concatenate(keys, axis=0)
        values = jnp.concatenate(values, axis=1)
        same = jnp.concatenate(docs, axis=0) == qdoc[...]
        for h in range(2):
            s = nt(keys[:, 128 * h : 128 * h + 128], qx[h])
            s = jnp.where(same, s, MASKED)
            old = top[h]
            new = jnp.maximum(old, jnp.max(s, axis=0, keepdims=True))
            p = jnp.exp2(s * SCALE_2 - new * SCALE_2)
            fade = jnp.exp2((old - new) * SCALE_2)
            top[h] = new
            total[h] = total[h] * fade + jnp.sum(p, axis=0, keepdims=True)
            acc[h] = acc[h] * fade + nn(values[64 * h : 64 * h + 64], p.astype(BF16))

    def units(count, place):
        def one(i, carry):
            unit(*place(i))
            return carry

        lax.fori_loop(0, count, one, 0)

    for a in range(4):
        partner(0, a)
    units(8, lambda i: (i // 4, 0, i % 4))
    for a in range(4):
        near(a)
        partner(1, a)
        partner(2, a)
        units(4, lambda i: (i // 2, 1 + i % 2, a))
    for a in range(4):
        far(a)
        partner(3, a)
        units(2, lambda i: (i, 3, a))

    rows = []
    for h in range(2):
        rows.append(acc[h] / total[h])
    attended = jnp.transpose(jnp.concatenate(rows, axis=0)).astype(BF16)
    logs = [top[h] * SCALE + jnp.log(total[h]) for h in range(2)]
    logs = jnp.transpose(jnp.concatenate(logs + [jnp.zeros((126, 256), F32)], axis=0))
    log_sums[...] = logs[:, 0:2]
    summed = nt(attended, w_out[...]).astype(BF16)
    partial[...] = summed.reshape(8, 32, 1024)
    for i, (dy, flip) in enumerate(tp_peers):
        target = ((y + dy) % 4) * 2 + (1 - c if flip else c)
        push(partial.at[target], rsbuf.at[i], send_t.at[7 + i], recv_t.at[7 + i], chip(dy=dy, flip=flip))
    out = partial[pl.ds(tp, 1)][0].astype(F32)
    for i in range(7):
        landed(rsbuf.at[i], recv_t.at[7 + i])
        out = out + rsbuf[i].astype(F32)
    mixed[...] = normed(out, out_gain[...]).astype(BF16)
    for copy in started:
        copy.wait_send()


def local(
    tokens,
    doc_ids,
    down_query,
    down_key,
    down_rotary,
    query_gain,
    key_gain,
    up_query,
    up_key,
    up_value,
    output_weight,
    out_gain,
):
    sp = lax.axis_index("sp")
    tp = lax.axis_index("tp")
    y, c = tp // 2, tp % 2
    half = jnp.where(c == 0, down_query, down_key)
    wpiece = lax.dynamic_slice_in_dim(half, 8 * y, 8, 0).reshape(8, 2, 128).transpose(1, 0, 2)
    uq = up_query.reshape(8, 2, 96)
    uq = jnp.concatenate([uq, uq[..., 80:96], uq[..., 64:80]], axis=-1).transpose(1, 0, 2)
    rot = down_rotary.reshape(4, 8, 32).transpose(1, 0, 2).reshape(1, 8, 128)
    wo = output_weight.T.reshape(4, 8, 128)
    bundle = jnp.concatenate([uq, up_key[None], up_value[None], rot, wo], axis=0)
    docs = doc_ids.astype(F32)
    own_docs = lax.dynamic_slice_in_dim(docs, 32 * tp, 32, 0)
    lane = jnp.arange(128)
    kdoc = jnp.where(lane == 32, own_docs[:16, None], jnp.where(lane == 96, own_docs[16:, None], 0.0))
    inverse = THETA ** (-(lane % 16).astype(F32) / 16)
    positions = sp * 256 + jnp.arange(256, dtype=jnp.int32)
    angles = positions.astype(F32)[:, None] * inverse[None, :]
    cosine, sine = jnp.cos(angles), jnp.sin(angles)
    signed = jnp.where(lane % 32 < 16, -sine, sine)
    turned = (lane >= 64) & (lane < 96)
    cos_q = jnp.where(lane < 64, 1.0, jnp.where(turned, cosine, 0.0))
    sin_q = jnp.where(turned, signed, 0.0)
    cos_k = lax.dynamic_slice_in_dim(cosine, 32 * tp, 32, 0)
    sin_k = lax.dynamic_slice_in_dim(signed, 32 * tp, 32, 0)
    dma = pltpu.SemaphoreType.DMA
    vm = pltpu.VMEM
    mixed, log_sums = pl.pallas_call(
        body,
        out_shape=(jax.ShapeDtypeStruct((32, 1024), BF16), jax.ShapeDtypeStruct((256, 2), F32)),
        in_specs=[pl.BlockSpec(memory_space=pltpu.VMEM)] * 12,
        out_specs=(pl.BlockSpec(memory_space=pltpu.VMEM),) * 2,
        scratch_shapes=[
            vm((2, 4, 4, 8, 2, 8, 128), BF16),
            vm((4, 8, 9, 8, 128), BF16),
            vm((2, 4, 4, 8, 80, 128), BF16),
            vm((8, 32, 256), BF16),
            vm((1024, 512), BF16),
            vm((1024, 128), BF16),
            vm((256, 256), BF16),
            vm((256, 128), F32),
            vm((256, 128), F32),
            vm((1024, 128), BF16),
            vm((2, 384, 256), BF16),
            vm((128, 256), BF16),
            vm((2, 256, 128), BF16),
            vm((2, 1, 256), F32),
            vm((2, 1, 256), F32),
            vm((2, 64, 256), F32),
            vm((8, 32, 1024), BF16),
            vm((7, 32, 1024), BF16),
            dma((2, 7)),
            dma((2, 7)),
            dma((12,)),
            dma((12,)),
            dma((48,)),
            dma((48,)),
            dma((64,)),
            dma((64,)),
            dma((7,)),
            dma((7,)),
            dma((4,)),
            dma((4,)),
            dma((14,)),
            dma((14,)),
        ],
        compiler_params=pltpu.CompilerParams(
            collective_id=0, has_side_effects=True, vmem_limit_bytes=40 * 1024 * 1024
        ),
    )(
        tokens,
        wpiece,
        bundle,
        docs.reshape(1, 256),
        kdoc,
        cos_q,
        sin_q,
        cos_k,
        sin_k,
        query_gain.reshape(1, 256),
        key_gain.reshape(1, 256),
        out_gain.reshape(1, 1024),
    )
    return mixed, log_sums


def solution(mesh):
    both = ("sp", "tp")
    return jax.shard_map(
        local,
        mesh=mesh,
        in_specs=(
            P(both, None),
            P("sp"),
            P("sp", None),
            P("sp", None),
            P("sp", None),
            P(),
            P(),
            P("sp", "tp"),
            P("sp", "tp"),
            P("sp", "tp"),
            P("tp", "sp"),
            P(),
        ),
        out_specs=(P(both, None), P("sp", "tp")),
        check_vma=False,
    )
```

```python
import functools
import math

import jax
import jax.numpy as jnp
from jax import lax
from jax.experimental import pallas as pl
from jax.experimental.pallas import tpu as pltpu
from jax.sharding import PartitionSpec as P

NOPE = 64
ROPE = 32
THETA = 10000.0
EPS = 1e-06
UNSEEN = -(2.0**97)
APART = -(2.0**100)
SCALE = 1.0 / math.sqrt(NOPE + ROPE)
SCALE_2 = SCALE * math.log2(math.e)
MESH = pl.DeviceIdType.MESH
F32 = jnp.float32
BF16 = jnp.bfloat16

STEPS = (0, 1, -1, 2, -2, 3, -3, 4)
SLOT_OF = {0: 0, 1: 1, -1: 2, 2: 3, -2: 4, 3: 5, -3: 6, 4: 7, -4: 7}
GROUPS = ((0, 4), (4, 4))


def slot8(r):
    late = r // 5
    return (1 - late) * (2 * r - 1 + (8 - r) // 8) + late * (16 - 2 * r)


def slot4(r):
    return 2 * r - r // 2 - 4 * (r // 3)


def nt(a, b):
    return lax.dot_general(a, b, (((1,), (1,)), ((), ())), preferred_element_type=F32)


def nn(a, b):
    return jnp.dot(a, b, preferred_element_type=F32)


def body(
    tok,
    wpiece,
    bundle,
    qdoc,
    kdoc,
    cos_q,
    sin_q,
    cos_k,
    sin_k,
    query_gain,
    key_gain,
    out_gain,
    mixed,
    log_sums,
    wbuf,
    bbuf,
    kbuf,
    qlbuf,
    w_down,
    w_rot,
    w_uq,
    w_uk,
    w_uv,
    w_out,
    kx_w,
    vt_w,
    qx,
    top,
    total,
    acc,
    partial,
    rsbuf,
    send_z,
    recv_z,
    send_2,
    recv_2,
    send_3,
    recv_3,
    send_p,
    recv_p,
    send_bz,
    recv_bz,
    send_bx,
    recv_bx,
    send_t,
    recv_t,
):
    sp = lax.axis_index("sp")
    tp = lax.axis_index("tp")
    z, x = sp // 4, sp % 4
    y, c = tp // 2, tp % 2

    def chip(dz=0, dx=0, dy=0, flip=False):
        core = 1 - c if flip else c
        return (((z + dz + 8) % 8) * 4 + (x + dx + 4) % 4, ((y + dy + 4) % 4) * 2 + core)

    def along_2(d):
        return chip(dx=(1 - c) * d, dy=c * d)

    def along_3(d):
        return chip(dx=c * d, dy=(1 - c) * d)

    tp_peers = [(dy, flip) for dy in (1, 3, 2, 0) for flip in (False, True) if (dy, flip) != (0, False)]

    barrier = pltpu.get_barrier_semaphore()
    peers = [chip(dz=d) for d in STEPS[1:]] + [chip(dx=1), chip(dx=-1)]
    peers += [chip(dy=dy, flip=flip) for dy, flip in tp_peers]
    for peer in peers:
        pl.semaphore_signal(barrier, inc=1, device_id=peer, device_id_type=MESH)
    pl.semaphore_wait(barrier, len(peers))

    started = []

    def push(src, dst, ssem, rsem, peer):
        copy = pltpu.make_async_remote_copy(
            src_ref=src, dst_ref=dst, send_sem=ssem, recv_sem=rsem, device_id=peer, device_id_type=MESH
        )
        copy.start()
        started.append(copy)

    def landed(dst, rsem):
        pltpu.make_async_remote_copy(
            src_ref=dst, dst_ref=dst, send_sem=rsem, recv_sem=rsem, device_id=chip(flip=True), device_id_type=MESH
        ).wait_recv()

    def spread(ids, buf, first):
        n2, n3 = 6 * ids, 24 * ids

        def go_z():
            for k in range(1, 8):
                slot = SLOT_OF[-STEPS[k]]
                push(first, buf.at[0, 0, 0, slot], send_z.at[ids, k - 1], recv_z.at[ids, slot - 1], chip(dz=STEPS[k]))

        def wait_z(g):
            lo, n = GROUPS[g]
            for k in range(max(lo, 1), lo + n):
                landed(buf.at[0, 0, 0, k], recv_z.at[ids, k - 1])

        def send_2nd(a_from, a_to, g, d):
            lo, n = GROUPS[g]
            i = n2 + (a_to - 1) * 2 + g
            push(buf.at[0, 0, a_from, pl.ds(lo, n)], buf.at[0, 0, a_to, pl.ds(lo, n)], send_2.at[i], recv_2.at[i], along_2(d))

        def wait_2nd(a, g):
            lo, n = GROUPS[g]
            landed(buf.at[0, 0, a, pl.ds(lo, n)], recv_2.at[n2 + (a - 1) * 2 + g])

        def send_3rd(b_from, b_to, a, g, d):
            lo, n = GROUPS[g]
            i = n3 + ((b_to - 1) * 4 + a) * 2 + g
            push(buf.at[0, b_from, a, pl.ds(lo, n)], buf.at[0, b_to, a, pl.ds(lo, n)], send_3.at[i], recv_3.at[i], along_3(d))

        def wait_3rd(b, a, g):
            lo, n = GROUPS[g]
            landed(buf.at[0, b, a, pl.ds(lo, n)], recv_3.at[n3 + ((b - 1) * 4 + a) * 2 + g])

        def share(b, a, g):
            lo, n = GROUPS[g]
            i = 32 * ids + (b * 4 + a) * 2 + g
            push(buf.at[0, b, a, pl.ds(lo, n)], buf.at[1, b, a, pl.ds(lo, n)], send_p.at[i], recv_p.at[i], chip(flip=True))

        def shared(b, a, g):
            lo, n = GROUPS[g]
            landed(buf.at[1, b, a, pl.ds(lo, n)], recv_p.at[32 * ids + (b * 4 + a) * 2 + g])

        def onward(a, g):
            send_3rd(0, 1, a, g, 1)
            send_3rd(0, 2, a, g, -1)
            share(0, a, g)

        def plane():
            for g in range(2):
                wait_z(g)
                send_2nd(0, 1, g, 1)
                send_2nd(0, 2, g, -1)
                onward(0, g)
            for g in range(2):
                wait_2nd(1, g)
                if g == 0:
                    send_2nd(1, 3, g, 1)
                onward(1, g)
                wait_2nd(2, g)
                if g == 1:
                    send_2nd(2, 3, g, -1)
                onward(2, g)
            for g in range(2):
                wait_2nd(3, g)
                onward(3, g)

        def near(a):
            for g in range(2):
                wait_3rd(1, a, g)
                if g == 0:
                    send_3rd(1, 3, a, g, 1)
                share(1, a, g)
                wait_3rd(2, a, g)
                if g == 1:
                    send_3rd(2, 3, a, g, -1)
                share(2, a, g)

        def far(a):
            for g in range(2):
                wait_3rd(3, a, g)
                share(3, a, g)

        def partner(b, a):
            for g in range(2):
                shared(b, a, g)

        return go_z, plane, near, far, partner

    go_z, plane, near, far, partner = spread(0, wbuf, wpiece)
    go_z()
    wbuf[0, 0, 0, 0] = wpiece[...]
    for k in range(1, 8):
        slot = SLOT_OF[-STEPS[k]]
        push(bundle, bbuf.at[0, slot], send_bz.at[k - 1], recv_bz.at[slot - 1], chip(dz=STEPS[k]))
    bbuf[0, 0] = bundle[...]
    plane()
    for k in range(1, 8):
        landed(bbuf.at[0, k], recv_bz.at[k - 1])
    for d, a in ((1, 1), (-1, 2)):
        push(bbuf.at[0], bbuf.at[a], send_bx.at[a - 1], recv_bx.at[a - 1], chip(dx=d))
    for a in range(4):
        near(a)
    for a in range(4):
        far(a)
    landed(bbuf.at[1], recv_bx.at[0])
    push(bbuf.at[1, pl.ds(0, 4)], bbuf.at[3, pl.ds(0, 4)], send_bx.at[2], recv_bx.at[2], chip(dx=1))
    landed(bbuf.at[2], recv_bx.at[1])
    push(bbuf.at[2, pl.ds(4, 4)], bbuf.at[3, pl.ds(4, 4)], send_bx.at[3], recv_bx.at[3], chip(dx=-1))
    for b in range(4):
        for a in range(4):
            partner(b, a)
    landed(bbuf.at[3, pl.ds(0, 4)], recv_bx.at[2])
    landed(bbuf.at[3, pl.ds(4, 4)], recv_bx.at[3])

    lane32 = lax.broadcasted_iota(jnp.int32, (1, 4, 1, 128), 3) // 32
    quarter = (lane32 == lax.broadcasted_iota(jnp.int32, (1, 4, 1, 128), 1)).astype(F32)[0]

    def arrange(s, carry):
        kz = slot8((s // 4 - z + 8) % 8)
        kx = slot4((s % 4 - x + 4) % 4)
        for half, first in ((0, c), (1, 1 - c)):
            for u in range(2):
                rows = []
                for yy in range(4):
                    ky = slot4((yy - y + 4) % 4)
                    b, a = (ky, kx) if half == 0 else (kx, ky)
                    rows.append(wbuf[first, b, a, kz, u].astype(F32))
                w_down[pl.ds(pl.multiple_of(s * 32, 32), 32), pl.ds((2 * half + u) * 128, 128)] = jnp.concatenate(
                    rows, axis=0
                ).astype(BF16)
        r = bbuf[kx, kz, 4].astype(F32)
        r = (r[None] * quarter).reshape(32, 128)
        w_rot[pl.ds(pl.multiple_of(s * 32, 32), 32), :] = r.astype(BF16)
        o = bbuf[kx, kz, pl.ds(5, 4)].astype(F32).reshape(32, 128)
        w_out[pl.ds(pl.multiple_of(s * 32, 32), 32), :] = o.astype(BF16)
        return carry

    lax.fori_loop(0, 32, arrange, 0)

    def arrange_up(s, carry):
        kz = slot8((s // 2 - z + 8) % 8)
        halves = [slot4((2 * (s % 2) + i - x + 4) % 4) for i in range(2)]
        at = pl.ds(pl.multiple_of(s * 16, 16), 16)
        for u in range(2):
            pair = [bbuf[kx, kz, u].astype(F32) for kx in halves]
            w_uq[at, pl.ds(u * 128, 128)] = jnp.concatenate(pair, axis=0).astype(BF16)
        w_uk[at, :] = jnp.concatenate([bbuf[kx, kz, 2].astype(F32) for kx in halves], axis=0)
        w_uv[at, :] = jnp.concatenate([bbuf[kx, kz, 3].astype(F32) for kx in halves], axis=0)
        return carry

    lax.fori_loop(0, 16, arrange_up, 0)

    own = tok[...]
    down = nn(own, w_down[...])

    def normed(v, gain):
        v = v.astype(BF16).astype(F32)
        return v * lax.rsqrt(jnp.mean(v * v, axis=-1, keepdims=True) + EPS) * gain

    latent_q = normed(down[:, :256], query_gain[...]).astype(BF16)
    latent_k = normed(down[:, 256:], key_gain[...]).astype(BF16)
    r = nn(own, w_rot[...])
    r = (r + pltpu.roll(r, 64, 1))
    r = (r + pltpu.roll(r, 32, 1)).astype(BF16).astype(F32)
    r = r * cos_k[...] + pltpu.roll(r, 16, 1) * sin_k[...]
    lane = lax.broadcasted_iota(jnp.int32, (16, 128), 1)
    turned = jnp.where(lane < 64, r[:16], r[16:])
    tail = jnp.where(lane % 64 < 32, turned, kdoc[...]).astype(BF16)
    kbuf[0, 0, 0, 0, pl.ds(0, 32)] = latent_k[:, :128]
    kbuf[0, 0, 0, 0, pl.ds(32, 32)] = latent_k[:, 128:]
    kbuf[0, 0, 0, 0, pl.ds(64, 16)] = tail
    qlbuf[pl.ds(tp, 1)] = latent_q[None]

    go_z, plane, near, far, partner = spread(1, kbuf, kbuf.at[0, 0, 0, 0])
    go_z()
    for i, (dy, flip) in enumerate(tp_peers):
        push(qlbuf.at[tp], qlbuf.at[tp], send_t.at[i], recv_t.at[i], chip(dy=dy, flip=flip))

    lane = lax.broadcasted_iota(jnp.int32, (256, 128), 1)
    uk = w_uk[...]
    head0 = jnp.where(lane < 64, uk, 0.0).astype(BF16)
    head1 = jnp.where(lane < 64, pltpu.roll(uk, 64, 1), 0.0).astype(BF16)
    row = lax.broadcasted_iota(jnp.int32, (128, 128), 0)
    col = lax.broadcasted_iota(jnp.int32, (128, 128), 1)
    for g in range(2):
        pick = ((row - 64 * g == col - 64) & (col >= 64)).astype(F32).astype(BF16)
        kx_w[g, pl.ds(0, 256), pl.ds(0, 128)] = head0
        kx_w[g, pl.ds(0, 256), pl.ds(128, 128)] = head1
        kx_w[g, pl.ds(256, 128), pl.ds(0, 128)] = pick
        kx_w[g, pl.ds(256, 128), pl.ds(128, 128)] = pick
    vt_w[...] = jnp.transpose(w_uv[...]).astype(BF16)
    top[...] = jnp.full_like(top, UNSEEN)
    total[...] = jnp.zeros_like(total)
    acc[...] = jnp.zeros_like(acc)

    plane()

    for i, (dy, flip) in enumerate(tp_peers):
        source = ((y + 4 - dy) % 4) * 2 + (1 - c if flip else c)
        landed(qlbuf.at[source], recv_t.at[i])
    q = nn(qlbuf[...].reshape(256, 256), w_uq[...]).astype(BF16).astype(F32)
    for h in range(2):
        v = q[:, 128 * h : 128 * h + 128]
        qx[h] = (v * cos_q[...] + pltpu.roll(v, 96, 1) * sin_q[...] + qdoc[...]).astype(BF16)

    def unit(side, b):
        block = kbuf[side, b]
        keys, values = [], []
        for g in range(2):
            low = block[:, :, 16 * g : 16 * g + 16].reshape(512, 128)
            high = block[:, :, 32 + 16 * g : 48 + 16 * g].reshape(512, 128)
            rest = block[:, :, 64:80].reshape(512, 128)
            keys.append(nn(jnp.concatenate([low, high, rest], axis=1), kx_w[g]).astype(BF16))
            values.append(nt(vt_w[...], jnp.concatenate([low, high], axis=1)).astype(BF16))
        keys = jnp.concatenate(keys, axis=0)
        values = jnp.concatenate(values, axis=1)
        for h in range(2):
            s = nt(keys[:, 128 * h : 128 * h + 128], qx[h])
            old = top[h]
            new = jnp.maximum(old, jnp.max(s, axis=0, keepdims=True))
            p = jnp.exp2(s * SCALE_2 - new * SCALE_2)
            fade = jnp.exp2((old - new) * SCALE_2)
            top[h] = new
            total[h] = total[h] * fade + jnp.sum(p, axis=0, keepdims=True)
            acc[h] = acc[h] * fade + nn(values[64 * h : 64 * h + 64], p.astype(BF16))

    def units(b):
        def one(i, carry):
            unit(i, b)
            return carry

        lax.fori_loop(0, 2, one, 0)

    for a in range(4):
        partner(0, a)
    units(0)
    for a in range(4):
        near(a)
    for b in (1, 2):
        for a in range(4):
            partner(b, a)
        units(b)
    for a in range(4):
        far(a)
    for a in range(4):
        partner(3, a)
    units(3)

    rows = []
    for h in range(2):
        rows.append(acc[h] / total[h])
    attended = jnp.transpose(jnp.concatenate(rows, axis=0)).astype(BF16)
    logs = [top[h] * SCALE + jnp.log(total[h]) for h in range(2)]
    logs = jnp.transpose(jnp.concatenate(logs + [jnp.zeros((126, 256), F32)], axis=0))
    log_sums[...] = logs[:, 0:2]
    summed = nt(attended, w_out[...]).astype(BF16)
    partial[...] = summed.reshape(8, 32, 1024)
    for i, (dy, flip) in enumerate(tp_peers):
        target = ((y + dy) % 4) * 2 + (1 - c if flip else c)
        push(partial.at[target], rsbuf.at[i], send_t.at[7 + i], recv_t.at[7 + i], chip(dy=dy, flip=flip))
    out = partial[pl.ds(tp, 1)][0].astype(F32)
    for i in range(7):
        landed(rsbuf.at[i], recv_t.at[7 + i])
        out = out + rsbuf[i].astype(F32)
    mixed[...] = normed(out, out_gain[...]).astype(BF16)
    for copy in started:
        copy.wait_send()


def local(
    tokens,
    doc_ids,
    down_query,
    down_key,
    down_rotary,
    query_gain,
    key_gain,
    up_query,
    up_key,
    up_value,
    output_weight,
    out_gain,
):
    sp = lax.axis_index("sp")
    tp = lax.axis_index("tp")
    y, c = tp // 2, tp % 2
    half = jnp.where(c == 0, down_query, down_key)
    wpiece = lax.dynamic_slice_in_dim(half, 8 * y, 8, 0).reshape(8, 2, 128).transpose(1, 0, 2)
    uq = up_query.reshape(8, 2, 96)
    uq = jnp.concatenate([uq, uq[..., 80:96], uq[..., 64:80]], axis=-1).transpose(1, 0, 2)
    rot = down_rotary.reshape(4, 8, 32).transpose(1, 0, 2).reshape(1, 8, 128)
    wo = output_weight.T.reshape(4, 8, 128)
    bundle = jnp.concatenate([uq, up_key[None], up_value[None], rot, wo], axis=0)
    docs = doc_ids.astype(F32)
    lane = jnp.arange(128)
    seen = docs[:, None] == (lane % 32).astype(F32)[None, :]
    qdoc = jnp.where(lane >= 96, jnp.where(seen, 0.0, APART), 0.0)
    own = lax.dynamic_slice_in_dim(seen, 32 * tp, 32, 0)
    kdoc = jnp.where(lane < 64, own[:16], own[16:]).astype(F32)
    inverse = THETA ** (-(lane % 16).astype(F32) / 16)
    positions = sp * 256 + jnp.arange(256, dtype=jnp.int32)
    angles = positions.astype(F32)[:, None] * inverse[None, :]
    cosine, sine = jnp.cos(angles), jnp.sin(angles)
    signed = jnp.where(lane % 32 < 16, -sine, sine)
    turned = (lane >= 64) & (lane < 96)
    cos_q = jnp.where(lane < 64, 1.0, jnp.where(turned, cosine, 0.0))
    sin_q = jnp.where(turned, signed, 0.0)
    cos_k = lax.dynamic_slice_in_dim(cosine, 32 * tp, 32, 0)
    sin_k = lax.dynamic_slice_in_dim(signed, 32 * tp, 32, 0)
    dma = pltpu.SemaphoreType.DMA
    vm = pltpu.VMEM
    mixed, log_sums = pl.pallas_call(
        body,
        out_shape=(jax.ShapeDtypeStruct((32, 1024), BF16), jax.ShapeDtypeStruct((256, 2), F32)),
        in_specs=[pl.BlockSpec(memory_space=pltpu.VMEM)] * 12,
        out_specs=(pl.BlockSpec(memory_space=pltpu.VMEM),) * 2,
        scratch_shapes=[
            vm((2, 4, 4, 8, 2, 8, 128), BF16),
            vm((4, 8, 9, 8, 128), BF16),
            vm((2, 4, 4, 8, 80, 128), BF16),
            vm((8, 32, 256), BF16),
            vm((1024, 512), BF16),
            vm((1024, 128), BF16),
            vm((256, 256), BF16),
            vm((256, 128), F32),
            vm((256, 128), F32),
            vm((1024, 128), BF16),
            vm((2, 384, 256), BF16),
            vm((128, 256), BF16),
            vm((2, 256, 128), BF16),
            vm((2, 1, 256), F32),
            vm((2, 1, 256), F32),
            vm((2, 64, 256), F32),
            vm((8, 32, 1024), BF16),
            vm((7, 32, 1024), BF16),
            dma((2, 7)),
            dma((2, 7)),
            dma((12,)),
            dma((12,)),
            dma((48,)),
            dma((48,)),
            dma((64,)),
            dma((64,)),
            dma((7,)),
            dma((7,)),
            dma((4,)),
            dma((4,)),
            dma((14,)),
            dma((14,)),
        ],
        compiler_params=pltpu.CompilerParams(
            collective_id=0, has_side_effects=True, vmem_limit_bytes=40 * 1024 * 1024
        ),
    )(
        tokens,
        wpiece,
        bundle,
        qdoc,
        kdoc,
        cos_q,
        sin_q,
        cos_k,
        sin_k,
        query_gain.reshape(1, 256),
        key_gain.reshape(1, 256),
        out_gain.reshape(1, 1024),
    )
    return mixed, log_sums


def solution(mesh):
    both = ("sp", "tp")
    return jax.shard_map(
        local,
        mesh=mesh,
        in_specs=(
            P(both, None),
            P("sp"),
            P("sp", None),
            P("sp", None),
            P("sp", None),
            P(),
            P(),
            P("sp", "tp"),
            P("sp", "tp"),
            P("sp", "tp"),
            P("tp", "sp"),
            P(),
        ),
        out_specs=(P(both, None), P("sp", "tp")),
        check_vma=False,
    )
```

```python
import functools
import math

import jax
import jax.numpy as jnp
from jax import lax
from jax.experimental import pallas as pl
from jax.experimental.pallas import tpu as pltpu
from jax.sharding import PartitionSpec as P

NOPE = 64
ROPE = 32
THETA = 10000.0
EPS = 1e-06
UNSEEN = -(2.0**97)
NOTHING = -1e30
APART = -(2.0**100)
SCALE = 1.0 / math.sqrt(NOPE + ROPE)
SCALE_2 = SCALE * math.log2(math.e)
MESH = pl.DeviceIdType.MESH
F32 = jnp.float32
BF16 = jnp.bfloat16

STEPS = (0, 1, -1, 2, -2, 3, -3, 4)
SLOT_OF = {0: 0, 1: 1, -1: 2, 2: 3, -2: 4, 3: 5, -3: 6, 4: 7, -4: 7}


K_GROUPS = ((0, 1), (1, 4), (5, 3))


def slot8(r):
    late = r // 5
    return (1 - late) * (2 * r - 1 + (8 - r) // 8) + late * (16 - 2 * r)


def slot4(r):
    return 2 * r - r // 2 - 4 * (r // 3)


def nt(a, b):
    return lax.dot_general(a, b, (((1,), (1,)), ((), ())), preferred_element_type=F32)


def nn(a, b):
    return jnp.dot(a, b, preferred_element_type=F32)


def body(
    tok,
    wpiece,
    rot,
    up,
    out_w,
    qdoc,
    kdoc,
    cos_q,
    sin_q,
    cos_k,
    sin_k,
    query_gain,
    key_gain,
    out_gain,
    mixed,
    log_sums,
    wbuf,
    rbuf,
    ubuf,
    obuf,
    kbuf,
    qlbuf,
    w_down,
    w_rot,
    w_uq,
    w_uk,
    w_uv,
    w_out,
    vt_w,
    qx,
    vt,
    top,
    total,
    acc,
    lbuf,
    shares,
    part_out,
    part_in,
    half_out,
    half_in,
    send_w,
    recv_w,
    send_r,
    recv_r,
    send_k,
    recv_k,
    send_t,
    recv_t,
):
    sp = lax.axis_index("sp")
    tp = lax.axis_index("tp")
    z, x = sp // 4, sp % 4
    y, c = tp // 2, tp % 2

    def chip(dz=0, dx=0, dy=0, flip=False):
        core = 1 - c if flip else c
        return (((z + dz + 8) % 8) * 4 + (x + dx + 4) % 4, ((y + dy + 4) % 4) * 2 + core)

    def along_2(d):
        return chip(dx=(1 - c) * d, dy=c * d)

    def along_3(d):
        return chip(dx=c * d, dy=(1 - c) * d)

    tp_peers = [(dy, flip) for dy in (1, 3, 2, 0) for flip in (False, True) if (dy, flip) != (0, False)]
    ring = ((1, 1), (2, -1), (3, 2))

    barrier = pltpu.get_barrier_semaphore()
    peers = [chip(dz=d) for d in STEPS[1:]] + [chip(dx=d) for _, d in ring]
    peers += [chip(dy=dy, flip=flip) for dy, flip in tp_peers]
    for peer in peers:
        pl.semaphore_signal(barrier, inc=1, device_id=peer, device_id_type=MESH)
    pl.semaphore_wait(barrier, len(peers))

    started = []

    def push(src, dst, ssem, rsem, peer):
        copy = pltpu.make_async_remote_copy(
            src_ref=src, dst_ref=dst, send_sem=ssem, recv_sem=rsem, device_id=peer, device_id_type=MESH
        )
        copy.start()
        started.append(copy)

    def landed(dst, rsem):
        pltpu.make_async_remote_copy(
            src_ref=dst, dst_ref=dst, send_sem=rsem, recv_sem=rsem, device_id=chip(flip=True), device_id_type=MESH
        ).wait_recv()

    def wide_z(i, buf, first):
        for k in range(1, 8):
            slot = SLOT_OF[-STEPS[k]]
            push(first, buf.at[0, 0, slot], send_w.at[i, k - 1], recv_w.at[i, slot - 1], chip(dz=STEPS[k]))

    def wide_2(i, buf):
        for k in range(1, 8):
            landed(buf.at[0, 0, k], recv_w.at[i, k - 1])
        for a, d in ring:
            push(buf.at[0, 0], buf.at[0, a], send_w.at[i, 6 + a], recv_w.at[i, 6 + a], along_2(d))

    def wide_3(i, buf):
        for a, d in ring:
            landed(buf.at[0, a], recv_w.at[i, 6 + a])
        for b, d in ring:
            push(buf.at[0], buf.at[b], send_w.at[i, 9 + b], recv_w.at[i, 9 + b], along_3(d))

    def wide_end(i, buf, b):
        landed(buf.at[b], recv_w.at[i, 9 + b])

    wbuf[0, 0, 0, 0] = wpiece[...]
    rbuf[0, 0] = rot[...]
    ubuf[0, 0, 0] = up[...]
    obuf[0, 0, 0] = out_w[...]
    ours, theirs = wbuf.at[0], wbuf.at[1]

    def share(i, at):
        push(at(ours), at(theirs), send_w.at[3, i], recv_w.at[3, i], chip(flip=True))

    wide_z(0, ours, wpiece)
    for a, d in ring:
        push(rot, rbuf.at[0, a], send_r.at[a - 1], recv_r.at[a - 1], chip(dx=d))
    wide_z(1, ubuf, up)
    wide_z(2, obuf, out_w)
    wide_2(0, ours)
    share(0, lambda w: w.at[0, 0])
    for a, d in ring:
        landed(rbuf.at[0, a], recv_r.at[a - 1])
    for k in range(1, 8):
        slot = SLOT_OF[-STEPS[k]]
        push(rbuf.at[0], rbuf.at[slot], send_r.at[2 + k], recv_r.at[2 + slot], chip(dz=STEPS[k]))
    wide_3(0, ours)
    share(1, lambda w: w.at[0, pl.ds(1, 3)])
    wide_2(1, ubuf)
    wide_2(2, obuf)
    for b in range(1, 4):
        wide_end(0, ours, b)
        share(1 + b, lambda w: w.at[b])
    wide_3(1, ubuf)
    for k in range(1, 8):
        landed(rbuf.at[k], recv_r.at[2 + k])
    landed(theirs.at[0, 0], recv_w.at[3, 0])
    landed(theirs.at[0, pl.ds(1, 3)], recv_w.at[3, 1])
    for b in range(1, 4):
        landed(theirs.at[b], recv_w.at[3, 1 + b])

    lane32 = lax.broadcasted_iota(jnp.int32, (1, 4, 1, 128), 3) // 32
    quarter = (lane32 == lax.broadcasted_iota(jnp.int32, (1, 4, 1, 128), 1)).astype(F32)[0]

    def slot_x(v):
        return slot4((v - x + 4) % 4)

    def slot_y(v):
        return slot4((v - y + 4) % 4)

    def arrange(s, carry):
        kz = slot8((s // 4 - z + 8) % 8)
        kx = slot_x(s % 4)
        for half, first in ((0, c), (1, 1 - c)):
            for u in range(2):
                rows = []
                for yy in range(4):
                    ky = slot_y(yy)
                    b, a = (ky, kx) if half == 0 else (kx, ky)
                    rows.append(wbuf[first, b, a, kz, u].astype(F32))
                w_down[pl.ds(pl.multiple_of(s * 32, 32), 32), pl.ds((2 * half + u) * 128, 128)] = jnp.concatenate(
                    rows, axis=0
                ).astype(BF16)
        r = rbuf[kz, kx].astype(F32)
        r = (r[None] * quarter).reshape(32, 128)
        w_rot[pl.ds(pl.multiple_of(s * 32, 32), 32), :] = r.astype(BF16)
        return carry

    lax.fori_loop(0, 32, arrange, 0)

    own = tok[...]
    down = nn(own, w_down[...])

    def normed(v, gain):
        v = v.astype(BF16).astype(F32)
        return v * lax.rsqrt(jnp.mean(v * v, axis=-1, keepdims=True) + EPS) * gain

    latent_q = normed(down[:, :256], query_gain[...]).astype(BF16)
    latent_k = normed(down[:, 256:], key_gain[...]).astype(BF16)
    r = nn(own, w_rot[...])
    r = r + pltpu.roll(r, 64, 1)
    r = (r + pltpu.roll(r, 32, 1)).astype(BF16).astype(F32)
    r = r * cos_k[...] + pltpu.roll(r, 16, 1) * sin_k[...]
    lane = lax.broadcasted_iota(jnp.int32, (16, 128), 1)
    turned = jnp.where(lane < 64, r[:16], r[16:])
    tail = jnp.where(lane % 64 < 32, turned, kdoc[...]).astype(BF16)
    kbuf[0, 0, 0, pl.ds(0, 32)] = latent_k[:, :128]
    kbuf[0, 0, 0, pl.ds(32, 32)] = latent_k[:, 128:]
    kbuf[0, 0, 0, pl.ds(64, 16)] = tail
    qlbuf[pl.ds(tp, 1)] = latent_q[None]

    def keys_x(g):
        lo, n = K_GROUPS[g]
        for k in range(max(lo, 1), lo + n):
            landed(kbuf.at[0, 0, k], recv_k.at[k - 1])
        run = pl.ds(lo, n)
        for a, d in ring:
            i = 7 + 3 * g + a - 1
            push(kbuf.at[0, 0, run], kbuf.at[0, a, run], send_k.at[i], recv_k.at[i], chip(dx=d))

    def keys_share(a):
        if a:
            for g, (lo, n) in enumerate(K_GROUPS):
                landed(kbuf.at[0, a, pl.ds(lo, n)], recv_k.at[7 + 3 * g + a - 1])
        push(kbuf.at[0, a], kbuf.at[1, a], send_k.at[16 + a], recv_k.at[16 + a], chip(flip=True))

    for k in range(1, 8):
        slot = SLOT_OF[-STEPS[k]]
        push(kbuf.at[0, 0, 0], kbuf.at[0, 0, slot], send_k.at[k - 1], recv_k.at[slot - 1], chip(dz=STEPS[k]))
    for i, (dy, flip) in enumerate(tp_peers):
        push(qlbuf.at[tp], qlbuf.at[tp], send_t.at[i], recv_t.at[i], chip(dy=dy, flip=flip))
    keys_x(0)
    for b in range(1, 4):
        wide_end(1, ubuf, b)

    def arrange_up(s, carry):
        kz = slot8((s // 2 - z + 8) % 8)
        at = pl.ds(pl.multiple_of(s * 16, 16), 16)
        for yy in range(4):
            ky = slot_y(yy)
            places = []
            for i in range(2):
                kx = slot_x(2 * (s % 2) + i)
                places.append(((1 - c) * ky + c * kx, (1 - c) * kx + c * ky))
            for u in range(4):
                v = jnp.concatenate([ubuf[b, a, kz, u].astype(F32) for b, a in places], axis=0)
                if u < 2:
                    w_uq[at, pl.ds((2 * yy + u) * 128, 128)] = v.astype(BF16)
                elif u == 2:
                    w_uk[yy, at, :] = v.astype(BF16)
                else:
                    w_uv[at, pl.ds(yy * 128, 128)] = v
        return carry

    def arrange_out(s, carry):
        kz = slot8((s // 4 - z + 8) % 8)
        kx = slot_x(s % 4)
        for yy in range(4):
            ky = slot_y(yy)
            o = obuf[(1 - c) * ky + c * kx, (1 - c) * kx + c * ky, kz].astype(F32).reshape(32, 128)
            w_out[pl.ds(pl.multiple_of(s * 32, 32), 32), pl.ds(yy * 128, 128)] = o.astype(BF16)
        return carry

    lax.fori_loop(0, 16, arrange_up, 0)
    vt_w[...] = jnp.transpose(w_uv[...]).astype(BF16)
    top[...] = jnp.full_like(top, UNSEEN)
    total[...] = jnp.zeros_like(total)
    acc[...] = jnp.zeros_like(acc)
    keys_x(1)

    for i, (dy, flip) in enumerate(tp_peers):
        source = ((y + 4 - dy) % 4) * 2 + (1 - c if flip else c)
        landed(qlbuf.at[source], recv_t.at[i])
    keys_x(2)
    keys_share(0)
    wide_3(2, obuf)
    lane = lax.broadcasted_iota(jnp.int32, (256, 128), 1)
    row = lax.broadcasted_iota(jnp.int32, (128, 128), 0)
    col = lax.broadcasted_iota(jnp.int32, (128, 128), 1)
    pick = [((row - 64 * g == col - 64) & (col >= 64)).astype(F32).astype(BF16) for g in range(2)]
    query_block = qlbuf[...].reshape(256, 256)

    def make_queries(yy, carry):
        for j in range(2):
            h = 2 * yy + j
            v = nn(query_block, w_uq[:, pl.ds(pl.multiple_of(h * 128, 128), 128)]).astype(BF16).astype(F32)
            rest = v * cos_q[...] + pltpu.roll(v, 96, 1) * sin_q[...] + qdoc[...]
            rest = jnp.where(lane < 64, 0.0, rest).astype(BF16)
            plain = jnp.where(lane < 64, v, 0.0)
            if j == 1:
                plain = pltpu.roll(plain, 64, 1)
            over = nt(w_uk[yy], plain.astype(BF16)).astype(BF16)
            for g in range(2):
                qx[g, h, pl.ds(0, 256)] = over
                qx[g, h, pl.ds(256, 128)] = nt(pick[g], rest).astype(BF16)
        return carry

    lax.fori_loop(0, 4, make_queries, 0)

    def attend(a):
        keys = []
        for g in range(2):
            low = kbuf[:, a, :, pl.ds(16 * g, 16)].reshape(256, 128)
            high = kbuf[:, a, :, pl.ds(32 + 16 * g, 16)].reshape(256, 128)
            rest = kbuf[:, a, :, pl.ds(64, 16)].reshape(256, 128)
            keys.append(jnp.concatenate([low, high, rest], axis=1))
            vt[:, pl.ds(256 * g, 256)] = nt(vt_w[...], keys[g][:, :256]).astype(BF16)

        def pair(i, carry):
            heads = [2 * i, 2 * i + 1]
            scores = [jnp.concatenate([nn(keys[g], qx[g, h]) for g in range(2)], axis=0) for h in heads]
            for h, s in zip(heads, scores):
                old = top[h]
                new = jnp.maximum(old, jnp.max(s, axis=0, keepdims=True))
                p = jnp.exp2(s * SCALE_2 - new * SCALE_2)
                fade = jnp.exp2((old - new) * SCALE_2)
                top[h] = new
                total[h] = total[h] * fade + jnp.sum(p, axis=0, keepdims=True)
                values = vt[pl.ds(pl.multiple_of(h * 64, 64), 64), :]
                acc[h] = acc[h] * fade + nn(values, p.astype(BF16))
            return carry

        lax.fori_loop(0, 4, pair, 0)

    landed(kbuf.at[1, 0], recv_k.at[16])
    attend(0)
    for a in range(1, 4):
        keys_share(a)
    for a in range(1, 4):
        landed(kbuf.at[1, a], recv_k.at[16 + a])
        attend(a)

    for h in range(8):
        seen = total[h] > 0.0
        lbuf[0, pl.ds(h, 1)] = jnp.where(seen, top[h] * SCALE_2 + jnp.log2(total[h]), NOTHING)
        acc[h] = acc[h] * jnp.where(seen, 1.0 / total[h], 0.0)
    for i, dy in ((1, 1), (2, 3), (3, 2)):
        push(lbuf.at[0], lbuf.at[i], send_t.at[6 + i], recv_t.at[6 + i], chip(dy=dy))
    part_out[...] = jnp.transpose(acc[...].reshape(512, 256)).astype(BF16).reshape(4, 64, 512)
    for i, dy in ((1, 1), (2, 3), (3, 2)):
        push(part_out.at[(y + dy) % 4], part_in.at[i - 1], send_t.at[9 + i], recv_t.at[9 + i], chip(dy=dy))
    for b in range(1, 4):
        wide_end(2, obuf, b)
    lax.fori_loop(0, 32, arrange_out, 0)
    for i in range(1, 4):
        landed(lbuf.at[i], recv_t.at[6 + i])
    logs = [lbuf[i] for i in range(4)]
    most = functools.reduce(jnp.maximum, logs)
    logs = [jnp.exp2(v - most) for v in logs]
    whole = sum(logs[1:], logs[0])
    logs = [v / whole for v in logs] + [(most + jnp.log2(whole)) * math.log(2.0)]
    flat = jnp.transpose(jnp.concatenate(logs + [jnp.zeros((88, 256), F32)], axis=0))
    shares[...] = flat.reshape(4, 64, 128)
    sums = [jnp.sum(jnp.where(lane == 32 + 2 * y + j, flat, 0.0), axis=1, keepdims=True) for j in range(2)]
    log_sums[...] = jnp.where(lane[:, 0:2] == 0, sums[0], sums[1])
    mine = shares[pl.ds(y, 1)][0]
    high = mine.astype(BF16)
    low = (mine - high.astype(F32)).astype(BF16)
    row = lax.broadcasted_iota(jnp.int32, (128, 512), 0)
    col = lax.broadcasted_iota(jnp.int32, (128, 512), 1)
    attended = jnp.zeros((64, 512), F32)
    for i in range(4):
        wide = (row == 8 * i + col // 64).astype(F32).astype(BF16)
        if i:
            landed(part_in.at[i - 1], recv_t.at[9 + i])
            part = part_in[i - 1]
        else:
            part = part_out[pl.ds(y, 1)][0]
        attended = attended + (nn(high, wide) + nn(low, wide)) * part.astype(F32)
    half_out[...] = nt(attended.astype(BF16), w_out[...]).reshape(2, 32, 1024).astype(BF16)
    push(half_out.at[1 - c], half_in, send_t.at[13], recv_t.at[13], chip(flip=True))
    out = half_out[pl.ds(c, 1)][0].astype(F32)
    landed(half_in, recv_t.at[13])
    mixed[...] = normed(out + half_in[...].astype(F32), out_gain[...]).astype(BF16)
    for copy in started:
        copy.wait_send()


def local(
    tokens,
    doc_ids,
    down_query,
    down_key,
    down_rotary,
    query_gain,
    key_gain,
    up_query,
    up_key,
    up_value,
    output_weight,
    out_gain,
):
    sp = lax.axis_index("sp")
    tp = lax.axis_index("tp")
    y, c = tp // 2, tp % 2
    half = jnp.where(c == 0, down_query, down_key)
    wpiece = lax.dynamic_slice_in_dim(half, 8 * y, 8, 0).reshape(8, 2, 128).transpose(1, 0, 2)
    uq = up_query.reshape(8, 2, 96)
    uq = jnp.concatenate([uq, uq[..., 80:96], uq[..., 64:80]], axis=-1).transpose(1, 0, 2)
    rot = down_rotary.reshape(4, 8, 32).transpose(1, 0, 2).reshape(8, 128)
    wo = output_weight.T.reshape(4, 8, 128)
    up = jnp.concatenate([uq, up_key[None], up_value[None]], axis=0)
    docs = doc_ids.astype(F32)
    lane = jnp.arange(128)
    seen = docs[:, None] == (lane % 32).astype(F32)[None, :]
    qdoc = jnp.where(lane >= 96, jnp.where(seen, 0.0, APART), 0.0)
    own = lax.dynamic_slice_in_dim(seen, 32 * tp, 32, 0)
    kdoc = jnp.where(lane < 64, own[:16], own[16:]).astype(F32)
    inverse = THETA ** (-(lane % 16).astype(F32) / 16)
    positions = sp * 256 + jnp.arange(256, dtype=jnp.int32)
    angles = positions.astype(F32)[:, None] * inverse[None, :]
    cosine, sine = jnp.cos(angles), jnp.sin(angles)
    signed = jnp.where(lane % 32 < 16, -sine, sine)
    turned = (lane >= 64) & (lane < 96)
    cos_q = jnp.where(lane < 64, 1.0, jnp.where(turned, cosine, 0.0))
    sin_q = jnp.where(turned, signed, 0.0)
    cos_k = lax.dynamic_slice_in_dim(cosine, 32 * tp, 32, 0)
    sin_k = lax.dynamic_slice_in_dim(signed, 32 * tp, 32, 0)
    dma = pltpu.SemaphoreType.DMA
    vm = pltpu.VMEM
    mixed, log_sums = pl.pallas_call(
        body,
        out_shape=(jax.ShapeDtypeStruct((32, 1024), BF16), jax.ShapeDtypeStruct((256, 2), F32)),
        in_specs=[pl.BlockSpec(memory_space=pltpu.VMEM)] * 14,
        out_specs=(pl.BlockSpec(memory_space=pltpu.VMEM),) * 2,
        scratch_shapes=[
            vm((2, 4, 4, 8, 2, 8, 128), BF16),
            vm((8, 4, 8, 128), BF16),
            vm((4, 4, 8, 4, 8, 128), BF16),
            vm((4, 4, 8, 4, 8, 128), BF16),
            vm((2, 4, 8, 80, 128), BF16),
            vm((8, 32, 256), BF16),
            vm((1024, 512), BF16),
            vm((1024, 128), BF16),
            vm((256, 1024), BF16),
            vm((4, 256, 128), BF16),
            vm((256, 512), F32),
            vm((1024, 512), BF16),
            vm((512, 256), BF16),
            vm((2, 8, 384, 256), BF16),
            vm((512, 512), BF16),
            vm((8, 1, 256), F32),
            vm((8, 1, 256), F32),
            vm((8, 64, 256), F32),
            vm((4, 8, 256), F32),
            vm((4, 64, 128), F32),
            vm((4, 64, 512), BF16),
            vm((3, 64, 512), BF16),
            vm((2, 32, 1024), BF16),
            vm((32, 1024), BF16),
            dma((4, 13)),
            dma((4, 13)),
            dma((10,)),
            dma((10,)),
            dma((20,)),
            dma((20,)),
            dma((14,)),
            dma((14,)),
        ],
        compiler_params=pltpu.CompilerParams(
            collective_id=0, has_side_effects=True, vmem_limit_bytes=40 * 1024 * 1024
        ),
    )(
        tokens,
        wpiece,
        rot,
        up,
        wo,
        qdoc,
        kdoc,
        cos_q,
        sin_q,
        cos_k,
        sin_k,
        query_gain.reshape(1, 256),
        key_gain.reshape(1, 256),
        out_gain.reshape(1, 1024),
    )
    return mixed, log_sums


def solution(mesh):
    both = ("sp", "tp")
    return jax.shard_map(
        local,
        mesh=mesh,
        in_specs=(
            P(both, None),
            P("sp"),
            P("sp", None),
            P("sp", None),
            P("sp", None),
            P(),
            P(),
            P("sp", "tp"),
            P("sp", "tp"),
            P("sp", "tp"),
            P("tp", "sp"),
            P(),
        ),
        out_specs=(P(both, None), P("sp", "tp")),
        check_vma=False,
    )
```

```python
import functools
import math

import jax
import jax.numpy as jnp
import numpy as np
from jax import lax
from jax.experimental import pallas as pl
from jax.experimental.pallas import tpu as pltpu
from jax.sharding import PartitionSpec as P

NOPE = 64
ROPE = 32
THETA = 10000.0
EPS = 1e-06
INVERSE = [float(v) for v in np.float32(THETA) ** (-np.arange(16, dtype=np.float32) / 16)]
UNSEEN = -(2.0**97)
NOTHING = -1e30
APART = -(2.0**100)
SCALE = 1.0 / math.sqrt(NOPE + ROPE)
SCALE_2 = SCALE * math.log2(math.e)
MESH = pl.DeviceIdType.MESH
F32 = jnp.float32
BF16 = jnp.bfloat16

STEPS = (0, 1, -1, 2, -2, 3, -3, 4)
SLOT_OF = {0: 0, 1: 1, -1: 2, 2: 3, -2: 4, 3: 5, -3: 6, 4: 7, -4: 7}


K_GROUPS = ((0, 1), (1, 4), (5, 3))


def slot8(r):
    late = r // 5
    return (1 - late) * (2 * r - 1 + (8 - r) // 8) + late * (16 - 2 * r)


def slot4(r):
    return 2 * r - r // 2 - 4 * (r // 3)


def nt(a, b):
    return lax.dot_general(a, b, (((1,), (1,)), ((), ())), preferred_element_type=F32)


def nn(a, b):
    return jnp.dot(a, b, preferred_element_type=F32)


def body(
    tokens,
    down_query,
    down_key,
    down_rotary,
    up_query,
    up_key,
    up_value,
    output_weight,
    query_gain,
    key_gain,
    out_gain,
    doc_ids,
    mixed,
    log_sums,
    tok,
    rot_in,
    up_in,
    gain_q,
    gain_k,
    gain_o,
    docs,
    doc,
    qdoc,
    cosine,
    sine,
    wbuf,
    rbuf,
    ubuf,
    obuf,
    kbuf,
    qlbuf,
    w_down,
    w_rot,
    w_uq,
    w_uk,
    w_uv,
    w_out,
    vt_w,
    qx,
    vt,
    top,
    total,
    acc,
    scores_a,
    scores_b,
    highest_a,
    highest_b,
    lbuf,
    shares,
    part_out,
    part_in,
    half_out,
    half_in,
    send_w,
    recv_w,
    send_r,
    recv_r,
    send_k,
    recv_k,
    send_t,
    recv_t,
    fetch,
):
    sp = lax.axis_index("sp")
    tp = lax.axis_index("tp")
    z, x = sp // 4, sp % 4
    y, c = tp // 2, tp % 2

    def chip(dz=0, dx=0, dy=0, flip=False):
        core = 1 - c if flip else c
        return (((z + dz + 8) % 8) * 4 + (x + dx + 4) % 4, ((y + dy + 4) % 4) * 2 + core)

    def along_2(d):
        return chip(dx=(1 - c) * d, dy=c * d)

    def along_3(d):
        return chip(dx=c * d, dy=(1 - c) * d)

    tp_peers = [(dy, flip) for dy in (1, 3, 2, 0) for flip in (False, True) if (dy, flip) != (0, False)]
    ring = ((1, 1), (2, -1), (3, 2))

    barrier = pltpu.get_barrier_semaphore()
    peers = [chip(dz=d) for d in STEPS[1:]] + [chip(dx=d) for _, d in ring]
    peers += [chip(dy=dy, flip=flip) for dy, flip in tp_peers]
    for peer in peers:
        pl.semaphore_signal(barrier, inc=1, device_id=peer, device_id_type=MESH)

    def fetched(i, src, dst):
        copy = pltpu.make_async_copy(src, dst, fetch.at[i])
        copy.start()
        return copy

    for core, weight in ((0, down_query), (1, down_key)):

        @pl.when(c == core)
        def _(weight=weight):
            for u in range(2):
                at = (pl.ds(pl.multiple_of(8 * y, 8), 8), pl.ds(128 * u, 128))
                fetched(u, weight.at[at], wbuf.at[0, 0, 0, 0, u])

    pairs = ((down_rotary, rot_in), (up_query, up_in), (up_key, ubuf.at[0, 0, 0, 2]))
    pairs += tuple((output_weight.at[pl.ds(8 * i, 8)], obuf.at[0, 0, 0, i]) for i in range(4))
    pairs += ((up_value, ubuf.at[0, 0, 0, 3]), (tokens, tok), (query_gain, gain_q), (key_gain, gain_k))
    pairs += ((out_gain, gain_o), (doc_ids, docs))
    copies = [fetched(2 + i, src, dst) for i, (src, dst) in enumerate(pairs)]
    for copy in copies[:2]:
        copy.wait()
    lane = lax.broadcasted_iota(jnp.int32, (8, 128), 1)
    row = lax.broadcasted_iota(jnp.int32, (32, 128), 0)
    col = lax.broadcasted_iota(jnp.int32, (32, 128), 1)
    r = nn(rot_in[...], (row == col % 32).astype(F32).astype(BF16))
    r = [jnp.where(lane // 32 == g, r[8 * g : 8 * g + 8], 0.0) for g in range(4)]
    rbuf[0, 0] = (r[0] + r[1] + r[2] + r[3]).astype(BF16)
    u0 = up_in[:, 0:128].astype(F32)
    u1 = jnp.concatenate([up_in[:, 128:192].astype(F32), jnp.zeros((8, 64), F32)], axis=1)
    u1 = jnp.where(lane < 32, pltpu.roll(u0, 32, 1), pltpu.roll(u1, 32, 1))
    for j, u in enumerate((u0, u1)):
        u = jnp.where(lane < 96, u, jnp.where(lane < 112, pltpu.roll(u, 16, 1), pltpu.roll(u, 48, 1)))
        ubuf[0, 0, 0, j] = u.astype(BF16)
    for i in range(2):
        pltpu.make_async_copy(wbuf.at[0, 0, 0, 0, i], wbuf.at[0, 0, 0, 0, i], fetch.at[i]).wait()
    for copy in copies[2:]:
        copy.wait()
    pl.semaphore_wait(barrier, len(peers))

    started = []

    def push(src, dst, ssem, rsem, peer):
        copy = pltpu.make_async_remote_copy(
            src_ref=src, dst_ref=dst, send_sem=ssem, recv_sem=rsem, device_id=peer, device_id_type=MESH
        )
        copy.start()
        started.append(copy)

    def landed(dst, rsem):
        pltpu.make_async_remote_copy(
            src_ref=dst, dst_ref=dst, send_sem=rsem, recv_sem=rsem, device_id=chip(flip=True), device_id_type=MESH
        ).wait_recv()

    def wide_z(i, buf):
        first = buf.at[0, 0, 0]
        for k in range(1, 8):
            slot = SLOT_OF[-STEPS[k]]
            push(first, buf.at[0, 0, slot], send_w.at[i, k - 1], recv_w.at[i, slot - 1], chip(dz=STEPS[k]))

    def wide_2(i, buf):
        for k in range(1, 8):
            landed(buf.at[0, 0, k], recv_w.at[i, k - 1])
        for a, d in ring:
            push(buf.at[0, 0], buf.at[0, a], send_w.at[i, 6 + a], recv_w.at[i, 6 + a], along_2(d))

    def wide_3(i, buf):
        for a, d in ring:
            landed(buf.at[0, a], recv_w.at[i, 6 + a])
        for b, d in ring:
            push(buf.at[0], buf.at[b], send_w.at[i, 9 + b], recv_w.at[i, 9 + b], along_3(d))

    def wide_end(i, buf, b):
        landed(buf.at[b], recv_w.at[i, 9 + b])

    ours, theirs = wbuf.at[0], wbuf.at[1]

    def share(i, at):
        push(at(ours), at(theirs), send_w.at[3, i], recv_w.at[3, i], chip(flip=True))

    wide_z(0, ours)
    for a, d in ring:
        push(rbuf.at[0, 0], rbuf.at[0, a], send_r.at[a - 1], recv_r.at[a - 1], chip(dx=d))
    wide_z(1, ubuf)
    wide_z(2, obuf)

    lane = lax.broadcasted_iota(jnp.int32, (1, 128), 1) % 16
    inverse = sum(jnp.where(lane == i, v, 0.0) for i, v in enumerate(INVERSE))
    angles = (sp * 256 + lax.broadcasted_iota(jnp.int32, (256, 128), 0)).astype(F32) * inverse
    lane = lax.broadcasted_iota(jnp.int32, (256, 128), 1)
    cosine[...] = jnp.cos(angles).reshape(8, 32, 128)
    sine[...] = (jnp.where(lane % 32 < 16, -1.0, 1.0) * jnp.sin(angles)).reshape(8, 32, 128)
    for i in range(2):
        turned = jnp.transpose(jnp.broadcast_to(docs[i : i + 1, :].astype(F32), (128, 128)))
        doc[pl.ds(4 * i, 4)] = turned.reshape(4, 32, 128)
    lane = lax.broadcasted_iota(jnp.int32, (256, 128), 1)
    apart = jnp.where(doc[...].reshape(256, 128) == (lane - 96).astype(F32), 0.0, APART)
    qdoc[...] = jnp.where(lane < 96, 0.0, apart)

    wide_2(0, ours)
    share(0, lambda w: w.at[0, 0])
    for a, d in ring:
        landed(rbuf.at[0, a], recv_r.at[a - 1])
    for k in range(1, 8):
        slot = SLOT_OF[-STEPS[k]]
        push(rbuf.at[0], rbuf.at[slot], send_r.at[2 + k], recv_r.at[2 + slot], chip(dz=STEPS[k]))
    wide_3(0, ours)
    share(1, lambda w: w.at[0, pl.ds(1, 3)])
    wide_2(1, ubuf)
    wide_2(2, obuf)
    for b in range(1, 4):
        wide_end(0, ours, b)
        share(1 + b, lambda w: w.at[b])
    wide_3(1, ubuf)
    for k in range(1, 8):
        landed(rbuf.at[k], recv_r.at[2 + k])
    landed(theirs.at[0, 0], recv_w.at[3, 0])
    landed(theirs.at[0, pl.ds(1, 3)], recv_w.at[3, 1])
    for b in range(1, 4):
        landed(theirs.at[b], recv_w.at[3, 1 + b])

    lane32 = lax.broadcasted_iota(jnp.int32, (1, 4, 1, 128), 3) // 32
    quarter = (lane32 == lax.broadcasted_iota(jnp.int32, (1, 4, 1, 128), 1)).astype(F32)[0]

    def slot_x(v):
        return slot4((v - x + 4) % 4)

    def slot_y(v):
        return slot4((v - y + 4) % 4)

    def arrange(s, carry):
        kz = slot8((s // 4 - z + 8) % 8)
        kx = slot_x(s % 4)
        for half, first in ((0, c), (1, 1 - c)):
            for u in range(2):
                rows = []
                for yy in range(4):
                    ky = slot_y(yy)
                    b, a = (ky, kx) if half == 0 else (kx, ky)
                    rows.append(wbuf[first, b, a, kz, u].astype(F32))
                w_down[pl.ds(pl.multiple_of(s * 32, 32), 32), pl.ds((2 * half + u) * 128, 128)] = jnp.concatenate(
                    rows, axis=0
                ).astype(BF16)
        r = rbuf[kz, kx].astype(F32)
        r = (r[None] * quarter).reshape(32, 128)
        w_rot[pl.ds(pl.multiple_of(s * 32, 32), 32), :] = r.astype(BF16)
        return carry

    lax.fori_loop(0, 32, arrange, 0)

    own = tok[...]
    down = nn(own, w_down[...])

    def normed(v, gain):
        v = v.astype(BF16).astype(F32)
        return v * lax.rsqrt(jnp.mean(v * v, axis=-1, keepdims=True) + EPS) * gain

    latent_q = normed(down[:, :256], gain_q[...]).astype(BF16)
    latent_k = normed(down[:, 256:], gain_k[...]).astype(BF16)
    r = nn(own, w_rot[...])
    r = r + pltpu.roll(r, 64, 1)
    r = (r + pltpu.roll(r, 32, 1)).astype(BF16).astype(F32)
    r = r * cosine[pl.ds(tp, 1)][0] + pltpu.roll(r, 16, 1) * sine[pl.ds(tp, 1)][0]
    lane = lax.broadcasted_iota(jnp.int32, (16, 128), 1)
    turned = jnp.where(lane < 64, r[:16], r[16:])
    d = doc[pl.ds(tp, 1)][0]
    d = jnp.where(lane < 64, d[:16], d[16:]) == (lane % 32).astype(F32)
    tail = jnp.where(lane % 64 < 32, turned, d.astype(F32)).astype(BF16)
    kbuf[0, 0, 0, pl.ds(0, 32)] = latent_k[:, :128]
    kbuf[0, 0, 0, pl.ds(32, 32)] = latent_k[:, 128:]
    kbuf[0, 0, 0, pl.ds(64, 16)] = tail
    qlbuf[pl.ds(tp, 1)] = latent_q[None]

    def keys_x(g):
        lo, n = K_GROUPS[g]
        for k in range(max(lo, 1), lo + n):
            landed(kbuf.at[0, 0, k], recv_k.at[k - 1])
        run = pl.ds(lo, n)
        for a, d in ring:
            i = 7 + 3 * g + a - 1
            push(kbuf.at[0, 0, run], kbuf.at[0, a, run], send_k.at[i], recv_k.at[i], chip(dx=d))

    def keys_share(a):
        if a:
            for g, (lo, n) in enumerate(K_GROUPS):
                landed(kbuf.at[0, a, pl.ds(lo, n)], recv_k.at[7 + 3 * g + a - 1])
        push(kbuf.at[0, a], kbuf.at[1, a], send_k.at[16 + a], recv_k.at[16 + a], chip(flip=True))

    for k in range(1, 8):
        slot = SLOT_OF[-STEPS[k]]
        push(kbuf.at[0, 0, 0], kbuf.at[0, 0, slot], send_k.at[k - 1], recv_k.at[slot - 1], chip(dz=STEPS[k]))
    for i, (dy, flip) in enumerate(tp_peers):
        push(qlbuf.at[tp], qlbuf.at[tp], send_t.at[i], recv_t.at[i], chip(dy=dy, flip=flip))
    keys_x(0)
    for b in range(1, 4):
        wide_end(1, ubuf, b)

    def arrange_up(s, carry):
        kz = slot8((s // 2 - z + 8) % 8)
        at = pl.ds(pl.multiple_of(s * 16, 16), 16)
        for yy in range(4):
            ky = slot_y(yy)
            places = []
            for i in range(2):
                kx = slot_x(2 * (s % 2) + i)
                places.append(((1 - c) * ky + c * kx, (1 - c) * kx + c * ky))
            for u in range(4):
                v = jnp.concatenate([ubuf[b, a, kz, u].astype(F32) for b, a in places], axis=0)
                if u < 2:
                    w_uq[at, pl.ds((2 * yy + u) * 128, 128)] = v.astype(BF16)
                elif u == 2:
                    w_uk[yy, at, :] = v.astype(BF16)
                else:
                    w_uv[at, pl.ds(yy * 128, 128)] = v
        return carry

    def arrange_out(s, carry):
        kz = slot8((s // 4 - z + 8) % 8)
        kx = slot_x(s % 4)
        for yy in range(4):
            ky = slot_y(yy)
            o = obuf[(1 - c) * ky + c * kx, (1 - c) * kx + c * ky, kz].astype(F32).reshape(32, 128)
            w_out[pl.ds(pl.multiple_of(s * 32, 32), 32), pl.ds(yy * 128, 128)] = o.astype(BF16)
        return carry

    lax.fori_loop(0, 16, arrange_up, 0)
    vt_w[...] = jnp.transpose(w_uv[...]).astype(BF16)
    top[...] = jnp.full_like(top, UNSEEN)
    total[...] = jnp.zeros_like(total)
    acc[...] = jnp.zeros_like(acc)
    keys_x(1)

    for i, (dy, flip) in enumerate(tp_peers):
        source = ((y + 4 - dy) % 4) * 2 + (1 - c if flip else c)
        landed(qlbuf.at[source], recv_t.at[i])
    keys_x(2)
    keys_share(0)
    wide_3(2, obuf)
    lane = lax.broadcasted_iota(jnp.int32, (256, 128), 1)
    row = lax.broadcasted_iota(jnp.int32, (128, 128), 0)
    col = lax.broadcasted_iota(jnp.int32, (128, 128), 1)
    pick = [((row - 64 * g == col - 64) & (col >= 64)).astype(F32).astype(BF16) for g in range(2)]
    query_block = qlbuf[...].reshape(256, 256)

    def make_queries(yy, carry):
        for j in range(2):
            h = 2 * yy + j
            v = nn(query_block, w_uq[:, pl.ds(pl.multiple_of(h * 128, 128), 128)]).astype(BF16).astype(F32)
            turned = v * cosine[...].reshape(256, 128) + pltpu.roll(v, 96, 1) * sine[...].reshape(256, 128)
            turned = turned.astype(BF16).astype(F32) * SCALE_2
            rest = jnp.where((lane < 64) | (lane >= 96), qdoc[...], turned).astype(BF16)
            plain = jnp.where(lane < 64, v, 0.0)
            if j == 1:
                plain = pltpu.roll(plain, 64, 1)
            over = (nt(w_uk[yy], plain.astype(BF16)) * SCALE_2).astype(BF16)
            for g in range(2):
                qx[g, h, pl.ds(0, 256)] = over
                qx[g, h, pl.ds(256, 128)] = nt(pick[g], rest).astype(BF16)
        return carry

    lax.fori_loop(0, 4, make_queries, 0)

    def keys_of(a, g):
        low = kbuf[:, a, :, pl.ds(16 * g, 16)].reshape(256, 128)
        high = kbuf[:, a, :, pl.ds(32 + 16 * g, 16)].reshape(256, 128)
        return low, high, kbuf[:, a, :, pl.ds(64, 16)].reshape(256, 128)

    def attend(a):
        for g in range(2):
            vt[:, pl.ds(256 * g, 256)] = nt(vt_w[...], jnp.concatenate(keys_of(a, g)[:2], axis=1)).astype(BF16)

        def score(h, scores, highest):
            new = top[h]
            for g in range(2):
                s = nn(jnp.concatenate(keys_of(a, g), axis=1), qx[g, h])
                scores[pl.ds(256 * g, 256), :] = s
                new = jnp.maximum(new, jnp.max(s, axis=0, keepdims=True))
            highest[...] = new

        def weigh(h, scores, highest):
            new = highest[...]
            p = jnp.exp2(scores[...] - new)
            fade = jnp.exp2(top[h] - new)
            top[h] = new
            total[h] = total[h] * fade + jnp.sum(p, axis=0, keepdims=True)
            values = vt[pl.ds(64 * h if isinstance(h, int) else pl.multiple_of(h * 64, 64), 64), :]
            acc[h] = acc[h] * fade + nn(values, p.astype(BF16))

        def pair(i, carry):
            score(2 * i + 1, scores_b, highest_b)
            weigh(2 * i, scores_a, highest_a)
            score(2 * i + 2, scores_a, highest_a)
            weigh(2 * i + 1, scores_b, highest_b)
            return carry

        score(0, scores_a, highest_a)
        lax.fori_loop(0, 3, pair, 0)
        score(7, scores_b, highest_b)
        weigh(6, scores_a, highest_a)
        weigh(7, scores_b, highest_b)

    landed(kbuf.at[1, 0], recv_k.at[16])
    attend(0)
    for a in range(1, 4):
        keys_share(a)
    for a in range(1, 4):
        landed(kbuf.at[1, a], recv_k.at[16 + a])
        attend(a)

    for h in range(8):
        seen = total[h] > 0.0
        lbuf[0, pl.ds(h, 1)] = jnp.where(seen, top[h] + jnp.log2(total[h]), NOTHING)
        acc[h] = acc[h] * jnp.where(seen, 1.0 / total[h], 0.0)
    for i, dy in ((1, 1), (2, 3), (3, 2)):
        push(lbuf.at[0], lbuf.at[i], send_t.at[6 + i], recv_t.at[6 + i], chip(dy=dy))
    part_out[...] = jnp.transpose(acc[...].reshape(512, 256)).astype(BF16).reshape(4, 64, 512)
    for i, dy in ((1, 1), (2, 3), (3, 2)):
        push(part_out.at[(y + dy) % 4], part_in.at[i - 1], send_t.at[9 + i], recv_t.at[9 + i], chip(dy=dy))
    for b in range(1, 4):
        wide_end(2, obuf, b)
    lax.fori_loop(0, 32, arrange_out, 0)
    for i in range(1, 4):
        landed(lbuf.at[i], recv_t.at[6 + i])
    logs = [lbuf[i] for i in range(4)]
    most = functools.reduce(jnp.maximum, logs)
    logs = [jnp.exp2(v - most) for v in logs]
    whole = sum(logs[1:], logs[0])
    logs = [v / whole for v in logs]
    row = lax.broadcasted_iota(jnp.int32, (8, 256), 0)
    whole = (most + jnp.log2(whole)) * math.log(2.0)
    for j in range(2):
        log_sums[pl.ds(j, 1)] = jnp.sum(jnp.where(row == 2 * y + j, whole, 0.0), axis=0, keepdims=True)
    shares[...] = jnp.transpose(jnp.concatenate(logs + [jnp.zeros((96, 256), F32)], axis=0)).reshape(4, 64, 128)
    mine = shares[pl.ds(y, 1)][0]
    high = mine.astype(BF16)
    low = (mine - high.astype(F32)).astype(BF16)
    row = lax.broadcasted_iota(jnp.int32, (128, 512), 0)
    col = lax.broadcasted_iota(jnp.int32, (128, 512), 1)
    attended = jnp.zeros((64, 512), F32)
    for i in range(4):
        wide = (row == 8 * i + col // 64).astype(F32).astype(BF16)
        if i:
            landed(part_in.at[i - 1], recv_t.at[9 + i])
            part = part_in[i - 1]
        else:
            part = part_out[pl.ds(y, 1)][0]
        attended = attended + (nn(high, wide) + nn(low, wide)) * part.astype(F32)
    half_out[...] = nt(attended.astype(BF16), w_out[...]).reshape(2, 32, 1024).astype(BF16)
    push(half_out.at[1 - c], half_in, send_t.at[13], recv_t.at[13], chip(flip=True))
    out = half_out[pl.ds(c, 1)][0].astype(F32)
    landed(half_in, recv_t.at[13])
    mixed[...] = normed(out + half_in[...].astype(F32), gain_o[...]).astype(BF16)
    for copy in started:
        copy.wait_send()


def local(
    tokens,
    doc_ids,
    down_query,
    down_key,
    down_rotary,
    query_gain,
    key_gain,
    up_query,
    up_key,
    up_value,
    output_weight,
    out_gain,
):
    dma = pltpu.SemaphoreType.DMA
    vm = pltpu.VMEM
    mixed, log_sums = pl.pallas_call(
        body,
        out_shape=(jax.ShapeDtypeStruct((32, 1024), BF16), jax.ShapeDtypeStruct((2, 256), F32)),
        in_specs=[pl.BlockSpec(memory_space=pltpu.HBM)] * 12,
        out_specs=(pl.BlockSpec(memory_space=pltpu.VMEM),) * 2,
        scratch_shapes=[
            vm((32, 1024), BF16),
            vm((32, 32), BF16),
            vm((8, 192), BF16),
            vm((1, 256), F32),
            vm((1, 256), F32),
            vm((1, 1024), F32),
            vm((2, 128), jnp.int32),
            vm((8, 32, 128), F32),
            vm((256, 128), F32),
            vm((8, 32, 128), F32),
            vm((8, 32, 128), F32),
            vm((2, 4, 4, 8, 2, 8, 128), BF16),
            vm((8, 4, 8, 128), BF16),
            vm((4, 4, 8, 4, 8, 128), BF16),
            vm((4, 4, 8, 4, 8, 128), BF16),
            vm((2, 4, 8, 80, 128), BF16),
            vm((8, 32, 256), BF16),
            vm((1024, 512), BF16),
            vm((1024, 128), BF16),
            vm((256, 1024), BF16),
            vm((4, 256, 128), BF16),
            vm((256, 512), F32),
            vm((1024, 512), BF16),
            vm((512, 256), BF16),
            vm((2, 8, 384, 256), BF16),
            vm((512, 512), BF16),
            vm((8, 1, 256), F32),
            vm((8, 1, 256), F32),
            vm((8, 64, 256), F32),
            vm((512, 256), F32),
            vm((512, 256), F32),
            vm((1, 256), F32),
            vm((1, 256), F32),
            vm((4, 8, 256), F32),
            vm((4, 64, 128), F32),
            vm((4, 64, 512), BF16),
            vm((3, 64, 512), BF16),
            vm((2, 32, 1024), BF16),
            vm((32, 1024), BF16),
            dma((4, 13)),
            dma((4, 13)),
            dma((10,)),
            dma((10,)),
            dma((20,)),
            dma((20,)),
            dma((14,)),
            dma((14,)),
            dma((15,)),
        ],
        compiler_params=pltpu.CompilerParams(
            collective_id=0, has_side_effects=True, vmem_limit_bytes=62 * 1024 * 1024
        ),
    )(
        tokens,
        down_query,
        down_key,
        down_rotary,
        up_query,
        up_key,
        up_value,
        output_weight.T,
        query_gain.reshape(1, 256),
        key_gain.reshape(1, 256),
        out_gain.reshape(1, 1024),
        doc_ids.reshape(2, 128),
    )
    return mixed, log_sums.T


def solution(mesh):
    both = ("sp", "tp")
    return jax.shard_map(
        local,
        mesh=mesh,
        in_specs=(
            P(both, None),
            P("sp"),
            P("sp", None),
            P("sp", None),
            P("sp", None),
            P(),
            P(),
            P("sp", "tp"),
            P("sp", "tp"),
            P("sp", "tp"),
            P("tp", "sp"),
            P(),
        ),
        out_specs=(P(both, None), P("sp", "tp")),
        check_vma=False,
    )
```
